32 devices in a mesh: gr: 2 (over x), fs: 8 (over z, y), tp: 2 (over core).
Axes of the slice: x: 2, y: 2, z: 4, core: 2. Of those that a mesh axis runs over, the one named last changes fastest.
Arguments:
- tokens: bfloat16 [4096, 2048], P(('gr', 'fs', 'tp')), may hold values from -6 to 6
- norm_gain: float32 [2048], P(('gr', 'fs')), may hold values from 0.1 to 1.9
- up_weight: float32 [2048, 8192], P(('gr', 'fs'), 'tp'), may hold values from -0.125 to 0.125
- down_weight: float32 [8192, 2048], P(('gr', 'fs'), 'tp'), may hold values from -0.0625 to 0.0625
Outputs:
- served: bfloat16 [4096, 2048], P(('gr', 'fs', 'tp'))
- serve_up: bfloat16 [2048, 8192], P(None, 'fs')
- serve_down: bfloat16 [8192, 2048], P('fs')
The draws below stay inside these ranges and needn't reach their ends.
All inputs are finite; a program needn't handle non-finite values.
Results may differ from the reference program's by a relative error of at most 0.017.
Values may be sent and summed in bfloat16 or wider, within the bound.
A program may use at most 64 MiB of HBM per device.

```python
import jax
import jax.numpy as jnp
from jax import lax

D = 2048
FF = 8192
TOKENS = 4096
N_GR = 2
N_FS = 8


def level_of(stream_key, shape, pieces, least, top_value):
    factor_of = 1.0
    for position, blocks in pieces:
        draws = jax.random.uniform(jax.random.fold_in(jax.random.fold_in(stream_key, 6), position), (blocks,), jnp.float32, least / len(pieces), top_value / len(pieces))
        factor_of = factor_of * jnp.repeat(jnp.exp(draws), shape[position] // blocks).reshape((-1,) + (1,) * (len(shape) - 1 - position))
    return factor_of


def noise(key, dims, spread, reach, split=(), dtype=jnp.bfloat16):
    array = jax.random.normal(key, dims, jnp.float32) * spread
    if len(split) > 0:
        array = level_of(key, dims, split, -0.22, 0.18) * array
    return jnp.clip(array, min=-reach, max=reach).astype(dtype)


def setup_inputs(seed: int = 0) -> dict:
    key_list = jax.random.split(jax.random.key(seed), 5)
    return {
        "tokens": noise(key_list[0], (TOKENS, D), 1.0, 6.0, ((0, 32),)),
        "norm_gain": jnp.clip(1.0 + 0.18 * jax.random.normal(key_list[1], (D,), jnp.float32), 0.1, 1.9),
        "up_weight": noise(key_list[2], (D, FF), D ** -0.5, 0.125, ((0, 16), (1, 2)), jnp.float32),
        "down_weight": noise(key_list[3], (FF, D), FF ** -0.5, 0.0625, ((0, 16), (1, 2)), jnp.float32),
    }


def reference(tokens, norm_gain, up_weight, down_weight):
    segment = FF // (N_GR * N_FS)
    block = FF // N_FS
    scaled = (norm_gain[:, None] * up_weight).astype(jnp.bfloat16)
    serve_up = scaled.reshape(D, N_GR, N_FS, segment).transpose(0, 2, 1, 3).reshape(D, FF)
    rounded = down_weight.astype(jnp.bfloat16)
    serve_down = rounded.reshape(N_GR, N_FS, segment, D).transpose(1, 0, 2, 3).reshape(FF, D)
    values = tokens.astype(jnp.float32)
    normed = (values * lax.rsqrt(lax.optimization_barrier(jnp.mean(values * values, axis=1, keepdims=True)) + 1e-06)).astype(jnp.bfloat16)
    hidden = jnp.square(jax.nn.relu(jnp.dot(normed, serve_up, preferred_element_type=jnp.float32))).astype(jnp.bfloat16)
    hidden_blocks = hidden.reshape(hidden.shape[0], N_FS, block).transpose(1, 0, 2)
    down_blocks = serve_down.reshape(N_FS, block, D)

    def accumulate(total, pair):
        part = jnp.dot(pair[0], pair[1], preferred_element_type=jnp.float32).astype(jnp.bfloat16)
        part = lax.optimization_barrier(part)
        return (total + part.astype(jnp.float32), None)
    total, unused = lax.scan(accumulate, jnp.zeros((hidden.shape[0], D), jnp.float32), (hidden_blocks, down_blocks))
    return (total.astype(jnp.bfloat16), serve_up, serve_down)
```

```python
import functools

import jax
import jax.numpy as jnp
from jax import lax
from jax.experimental import pallas as pl
from jax.experimental.pallas import tpu as pltpu
from jax.sharding import PartitionSpec as P

MESH = pl.DeviceIdType.MESH
TILE = 512
STEP = 16


def inner_size(shards):
    return max(d for d in range(1, shards + 1) if shards % d == 0 and d * d <= shards)


def heavy_rows(rows, inner):
    return rows if inner == 1 else max(STEP, rows * 3 // 4 // STEP * STEP)


def kernel(sizes, normed, up, down, served, su, sd, tok, hid, part, got, far, lit, rest, *sems):
    groups, shards, cores = sizes
    inner = inner_size(shards)
    outer = shards // inner
    (up_send, up_recv, gu_send, gu_recv, tu_send, tu_recv, gd_send, gd_recv,
     td_send, td_recv, hop_send, hop_recv, light_send, light_recv, heavy_send, heavy_recv,
     near_send, near_recv, far_send, far_recv, lit_send, lit_recv, ou_send, ou_recv, local) = sems
    g, f, t = lax.axis_index("gr"), lax.axis_index("fs"), lax.axis_index("tp")
    z, y = f // inner, lax.rem(f, inner)
    rows, depth = normed.shape
    own_rows = up.shape[0]
    segment, dcols = down.shape
    nseg = up.shape[1] // segment
    group_rows = shards * own_rows
    width = su.shape[1]
    heavy = heavy_rows(rows, inner)
    light = rows - heavy
    front = rows + (inner - 1) * light
    stack = inner * rows
    half = rows // 2
    tiles = depth // TILE
    low, high = z > 0, z < outer - 1

    def to(axis, me, size, step):
        return {axis: lax.rem(me + step, size)}

    def rdma(src, dst, send, recv, device):
        return pltpu.make_async_remote_copy(
            src_ref=src, dst_ref=dst, send_sem=send, recv_sem=recv,
            device_id=device, device_id_type=MESH,
        )

    def back(i):
        return {"fs": z * inner + lax.rem(y + inner - i, inner)}

    def ahead(i):
        return {"fs": z * inner + lax.rem(y + i, inner)}

    def beside(step):
        return {"fs": (z + step) * inner + y}

    def span(ref, start, count, n=None):
        at = pl.ds(start if isinstance(start, int) else pl.multiple_of(start, STEP), count)
        if n is None:
            return ref.at[at]
        return ref.at[at, pl.ds(n * TILE if isinstance(n, int) else pl.multiple_of(n * TILE, TILE), TILE)]

    peers = [to("fs", f, shards, k) for k in range(1, shards)]
    peers += [to("gr", g, groups, k) for k in range(1, groups)]
    peers += [to("tp", t, cores, k) for k in range(1, cores)]
    barrier = pltpu.get_barrier_semaphore()
    for peer in peers:
        pl.semaphore_signal(barrier, inc=1, device_id=peer, device_id_type=MESH)
    pl.semaphore_wait(barrier, len(peers))

    def up_block(group, shard, sg):
        row = pl.multiple_of((group * shards + shard) * own_rows, own_rows)
        return su.at[pl.ds(row, own_rows), pl.ds(pl.multiple_of(sg * segment, segment), segment)]

    def up_group(group, sg):
        row = pl.multiple_of(group * group_rows, group_rows)
        return su.at[pl.ds(row, group_rows), pl.ds(sg * segment, segment)]

    def down_block(group, core):
        row = pl.multiple_of(group * segment, segment)
        return sd.at[pl.ds(row, segment), pl.ds(pl.multiple_of(core * dcols, dcols), dcols)]

    def owner(sg):
        return (sg * shards + f) // nseg

    sends = []

    def begin(copy):
        copy.start()
        sends.append(copy)

    down_in = []
    for k in range(1, groups):
        begin(rdma(down, down_block(g, t), gd_send.at[k], gd_recv.at[k], to("gr", g, groups, k)))
        down_in.append((k, lax.rem(g + groups - k, groups)))

    def up_copy(i):
        number = t * nseg + i
        shard, sg = lax.rem(number, shards), number // shards
        step = lax.rem(shard - f + shards, shards)
        src = up.at[:, pl.ds(pl.multiple_of(i * segment, segment), segment)]
        remote = rdma(src, up_block(g, f, sg), up_send.at[i], up_recv.at[sg, step], {"fs": shard})
        here = pltpu.make_async_copy(src, up_block(g, f, sg), up_recv.at[sg, 0])
        return shard == f, here, remote

    def start_up(j, carry):
        mine, here, remote = up_copy(lax.rem(f + j, nseg))
        pl.when(mine)(here.start)
        pl.when(jnp.logical_not(mine))(remote.start)
        return carry

    lax.fori_loop(0, nseg, start_up, 0)

    keep_down = pltpu.make_async_copy(down, down_block(g, t), local.at[0])
    keep_tok = pltpu.make_async_copy(normed, span(tok, 0, rows), local.at[1])
    keep_down.start()
    keep_tok.start()

    pieces = [(0, half), (half, rows - half)] + ([(rows, front - rows)] if front > rows else [])

    def hop(o, step, c):
        start, count = pieces[c]
        n = o + step
        own = o in (0, outer)
        src = span(normed, start, count) if own and c < 2 else span(tok, (o % outer) * stack + start, count)
        index = n if step > 0 else outer + n
        return rdma(src, span(tok, n * stack + start, count), hop_send.at[index, c], hop_recv.at[n, c], beside(step))

    hops = []

    def move(o, step, c, when):
        pl.when(when)(lambda: hop(o, step, c).start())
        hops.append((o, step, c, when))

    def light_copy(i):
        return rdma(span(normed, heavy, light), span(tok, rows + (i - 1) * light, light),
                    light_send.at[i], light_recv.at[i], ahead(i))

    def heavy_copy(n, i, c):
        start = 0 if c == 0 else half
        count = min(half, heavy) if c == 0 else heavy - half
        src = span(normed, start, count) if isinstance(n, int) and n == 0 else span(tok, n * stack + start, count)
        return rdma(src, span(tok, n * stack + front + (i - 1) * heavy + start, count),
                    heavy_send.at[n, i, c], heavy_recv.at[n, i, c], ahead(i))

    parts = (0, 1) if heavy > half else (0,)

    if light:
        for i in range(1, inner):
            begin(light_copy(i))
    for c in range(2):
        if outer > 1:
            move(0, 1, c, high)
            move(outer, -1, c, low)
    for c in parts:
        for i in range(1, inner):
            begin(heavy_copy(0, i, c))
    for k in range(1, cores):
        begin(rdma(down, down_block(g, t), td_send.at[k, 0], td_recv.at[k, 0], to("tp", t, cores, k)))

    for sg in range(groups):
        def forward(sg=sg):
            def arrived(k, carry):
                shard = lax.rem(f + shards - k, shards)
                block = up_block(g, shard, sg)

                @pl.when(k == 0)
                def _():
                    pltpu.make_async_copy(block, block, up_recv.at[sg, 0]).wait()

                @pl.when(k > 0)
                def _():
                    rdma(block, block, up_send.at[0], up_recv.at[sg, k], {"fs": shard}).wait_recv()

                for d in range(1, groups):
                    rdma(block, block, gu_send.at[sg, d, k], gu_recv.at[sg, d, k],
                         to("gr", g, groups, d)).start()
                return carry

            lax.fori_loop(0, shards, arrived, 0)
            whole = up_group(g, sg)
            for c in range(1, cores):
                rdma(whole, whole, tu_send.at[sg, 0, c], tu_recv.at[sg, 0], to("tp", t, cores, c)).start()

        pl.when(owner(sg) == t)(forward)

    if light:
        for i in range(1, inner):
            light_copy(i).wait_recv()
        if outer > 1:
            move(0, 1, 2, high)
            move(outer, -1, 2, low)

    def pass_on(o):
        for c in range(len(pieces)):
            for n, when, step, more in ((o, z >= o, 1, high), (outer - o, z + o < outer, -1, low)):
                start, count = pieces[c]
                block = span(tok, n * stack + start, count)

                @pl.when(when)
                def _(n=n, step=step, block=block, c=c):
                    rdma(block, block, hop_send.at[0, c], hop_recv.at[n, c], beside(-step)).wait_recv()

                if 0 < n + step < outer:
                    move(n, step, c, when & more)

                if c in parts:
                    @pl.when(when)
                    def _(n=n, c=c):
                        for i in range(1, inner):
                            heavy_copy(n, i, c).start()

    if outer > 1:
        pass_on(1)

    for k, source in down_in:
        block = down_block(source, t)
        rdma(block, block, gd_send.at[k], gd_recv.at[k], {"gr": source}).wait_recv()
        for c in range(1, cores):
            begin(rdma(block, block, td_send.at[c, k], td_recv.at[c, k], to("tp", t, cores, c)))

    def onward(first, last):
        for sg in range(groups):
            def relay(sg=sg):
                for d in range(1, groups):
                    source = lax.rem(g + groups - d, groups)

                    def arrived(k, carry):
                        block = up_block(source, lax.rem(f + shards - k, shards), sg)
                        rdma(block, block, gu_send.at[sg, d, k], gu_recv.at[sg, d, k], {"gr": source}).wait()
                        for c in range(1, cores):
                            rdma(block, block, ou_send.at[sg, d, c, k], ou_recv.at[sg, d, k],
                                 to("tp", t, cores, c)).start()
                        return carry

                    lax.fori_loop(first, last, arrived, 0)

            pl.when(owner(sg) == t)(relay)

    onward(0, shards // 2)
    if outer > 2:
        pass_on(2)
    early = outer == 4
    if not early:
        for o in range(3, outer):
            pass_on(o)
    onward(shards // 2, shards)

    keep_down.wait()
    keep_tok.wait()
    for c in range(1, cores):
        core = lax.rem(t + cores - c, cores)
        for k in range(groups):
            block = down_block(lax.rem(g + groups - k, groups), core)
            rdma(block, block, td_send.at[c, k], td_recv.at[c, k], {"tp": core}).wait_recv()
    for sg in range(groups):
        def take(sg=sg):
            whole = up_group(g, sg)
            rdma(whole, whole, tu_send.at[sg, 0, 1], tu_recv.at[sg, 0], {"tp": owner(sg)}).wait_recv()
            for d in range(1, groups):
                def taken(k, carry):
                    block = up_block(lax.rem(g + groups - d, groups), lax.rem(f + shards - k, shards), sg)
                    rdma(block, block, tu_send.at[sg, 0, 1], ou_recv.at[sg, d, k],
                         {"tp": owner(sg)}).wait_recv()
                    return carry

                lax.fori_loop(0, shards, taken, 0)

        pl.when(owner(sg) != t)(take)

    def near_copy(o, i, n):
        return rdma(span(part, o * stack + front + (i - 1) * heavy, heavy, n),
                    span(got, (o * (inner - 1) + i - 1) * heavy, heavy, n),
                    near_send.at[o, i, n], near_recv.at[o, i, n], back(i))

    def far_copy(o, n):
        right = o > z
        step = jnp.where(right, 1, -1)
        last = jnp.where(right, o == outer - 1, o == 1)
        slot = jnp.where(last, jnp.where(right, 0, outer), o + step)
        return rdma(span(part, o * stack, front, n), span(far, slot * front, front, n),
                    far_send.at[o, n], far_recv.at[slot, n], beside(step))

    def far_arrived(slot, step, n):
        block = span(far, slot * front, front, n)
        rdma(block, block, far_send.at[0, 0], far_recv.at[slot, n], beside(step)).wait_recv()

    def clear(slot):
        def zero(r, carry):
            far[pl.ds(pl.multiple_of(slot * front + r * STEP, STEP), STEP), :] = jnp.zeros((STEP, depth), jnp.bfloat16)
            return carry

        lax.fori_loop(0, front // STEP, zero, 0)

    def passes(o):
        right = o > z
        return (right & low) | (jnp.logical_not(right) & high)

    for o in range(1, outer):
        pl.when(jnp.logical_not(passes(o)))(lambda o=o: clear(o))
    pl.when(jnp.logical_not(low))(lambda: clear(0))
    pl.when(jnp.logical_not(high))(lambda: clear(outer))

    def compute(o):
        for i in range(1, inner):
            for c in parts:
                start = 0 if c == 0 else half
                count = min(half, heavy) if c == 0 else heavy - half
                block = span(tok, o * stack + front + (i - 1) * heavy + start, count)
                rdma(block, block, heavy_send.at[o, i, c], heavy_recv.at[o, i, c], back(i)).wait_recv()
        both = pl.ds(pl.multiple_of(o * stack, stack), stack)

        def first(n, carry):
            cols = pl.ds(pl.multiple_of(n * TILE, TILE), TILE)
            product = jnp.dot(tok[both, :], su[:, cols], preferred_element_type=jnp.float32)
            product = jnp.maximum(product, 0.0)
            hid[:, cols] = (product * product).astype(jnp.bfloat16)
            return carry

        lax.fori_loop(0, width // TILE, first, 0)

        def second(n, carry):
            cols = pl.ds(pl.multiple_of(n * TILE, TILE), TILE)
            product = jnp.dot(hid[...], sd[:, cols], preferred_element_type=jnp.float32)
            part[both, cols] = product.astype(jnp.bfloat16)
            for i in range(1, inner):
                near_copy(o, i, n).start()
            return carry

        lax.fori_loop(0, tiles, second, 0)

    def gather(o, n):
        for i in range(1, inner):
            near_copy(o, i, n).wait()

    def cells(start, n):
        return pl.ds(pl.multiple_of(start, STEP), STEP), pl.ds(pl.multiple_of(n * TILE, TILE), TILE)

    def value_at(o, r, n, ends, spread):
        value = part[cells(o * stack + r * STEP, n)].astype(jnp.float32)
        if spread:
            for i in range(1, inner):
                value += got[cells((o * (inner - 1) + i - 1) * heavy + r * STEP, n)].astype(jnp.float32)
        for end in ends:
            value += far[cells(end * front + r * STEP, n)].astype(jnp.float32)
        return value

    def add(o):
        def tile(n, carry):
            gather(o, n)

            @pl.when(passes(o))
            def _():
                far_arrived(o, jnp.where(o > z, -1, 1), n)

            def chunk(spread, r, carry):
                value = value_at(o, r, n, (o,), spread)
                part[cells(o * stack + r * STEP, n)] = value.astype(jnp.bfloat16)
                return carry

            lax.fori_loop(0, heavy // STEP, functools.partial(chunk, True), 0)
            lax.fori_loop(heavy // STEP, front // STEP, functools.partial(chunk, False), 0)
            far_copy(o, n).start()
            return carry

        lax.fori_loop(0, tiles, tile, 0)

    order = []
    left_end, right_end = z * 0, z * 0 + outer - 1
    for _ in range(outer):
        take_left = z - left_end > right_end - z
        owner_z = jnp.where(take_left, left_end, right_end)
        order.append(lax.rem(z - owner_z + outer, outer))
        left_end = jnp.where(take_left, left_end + 1, left_end)
        right_end = jnp.where(take_left, right_end, right_end - 1)
    if early:
        second_far, first_far, third_far, _ = order
        compute(first_far)
        compute(third_far)
        add(first_far)
        pass_on(3)
        compute(second_far)
        add(second_far)
        compute(0)
        add(third_far)
    else:
        for o in order[:-1]:
            compute(o)
        compute(0)
        for o in order[:-1]:
            add(o)

    def lit_copy(i, n):
        return rdma(span(part, rows + (i - 1) * light, light, n), span(lit, (i - 1) * light, light, n),
                    lit_send.at[i, n], lit_recv.at[i, n], back(i))

    def total(n, carry):
        gather(0, n)
        pl.when(low)(lambda: far_arrived(0, -1, n))
        pl.when(high)(lambda: far_arrived(outer, 1, n))
        ends = (0, outer)

        def others(r, carry):
            part[cells(r * STEP, n)] = value_at(0, r, n, ends, False).astype(jnp.bfloat16)
            return carry

        def half_done(r, carry):
            rest[cells((r * STEP - heavy), n)] = value_at(0, r, n, ends, False)
            return carry

        def done(r, carry):
            served[cells(r * STEP, n)] = value_at(0, r, n, ends, True).astype(jnp.bfloat16)
            return carry

        if light:
            lax.fori_loop(rows // STEP, front // STEP, others, 0)
            for i in range(1, inner):
                lit_copy(i, n).start()
            lax.fori_loop(heavy // STEP, rows // STEP, half_done, 0)
        lax.fori_loop(0, heavy // STEP, done, 0)
        return carry

    lax.fori_loop(0, tiles, total, 0)

    if light:
        def finish(n, carry):
            for i in range(1, inner):
                lit_copy(i, n).wait()

            def chunk(r, carry):
                value = rest[cells(r * STEP, n)]
                for i in range(1, inner):
                    value += lit[cells((i - 1) * light + r * STEP, n)].astype(jnp.float32)
                served[cells(heavy + r * STEP, n)] = value.astype(jnp.bfloat16)
                return carry

            lax.fori_loop(0, light // STEP, chunk, 0)
            return carry

        lax.fori_loop(0, tiles, finish, 0)

    for o, step, c, when in hops:
        pl.when(when)(lambda o=o, step=step, c=c: hop(o, step, c).wait_send())
    for n in range(1, outer):
        for c in parts:
            for i in range(1, inner):
                heavy_copy(n, i, c).wait_send()

        def gone(m, carry, n=n):
            far_copy(n, m).wait_send()
            return carry

        lax.fori_loop(0, tiles, gone, 0)
    for copy in sends:
        copy.wait_send()

    def end_up(j, carry):
        mine, here, remote = up_copy(j)
        pl.when(jnp.logical_not(mine))(remote.wait_send)
        return carry

    lax.fori_loop(0, nseg, end_up, 0)
    for sg in range(groups):
        def end(sg=sg):
            whole = up_group(g, sg)
            for c in range(1, cores):
                rdma(whole, whole, tu_send.at[sg, 0, c], tu_recv.at[sg, 0],
                     to("tp", t, cores, c)).wait_send()
            for d in range(1, groups):
                def left(k, carry):
                    block = up_block(lax.rem(g + groups - d, groups), lax.rem(f + shards - k, shards), sg)
                    for c in range(1, cores):
                        rdma(block, block, ou_send.at[sg, d, c, k], ou_recv.at[sg, d, k],
                             to("tp", t, cores, c)).wait_send()
                    return carry

                lax.fori_loop(0, shards, left, 0)

        pl.when(owner(sg) == t)(end)


def body(tokens, norm_gain, up_weight, down_weight):
    groups, shards, cores = (lax.axis_size(a) for a in ("gr", "fs", "tp"))
    segment = down_weight.shape[0]
    up = (norm_gain[:, None] * up_weight).astype(jnp.bfloat16)
    down = down_weight.astype(jnp.bfloat16)
    values = tokens.astype(jnp.float32)
    normed = (values * lax.rsqrt(jnp.mean(values * values, axis=1, keepdims=True) + 1e-06)).astype(
        jnp.bfloat16
    )
    rows, depth = tokens.shape
    inner = inner_size(shards)
    outer = shards // inner
    heavy = heavy_rows(rows, inner)
    light = rows - heavy
    front = rows + (inner - 1) * light
    nseg = up.shape[1] // segment
    width = groups * segment
    tiles = depth // TILE
    bf = jnp.bfloat16
    dma = pltpu.SemaphoreType.DMA
    vmem = pl.BlockSpec(memory_space=pltpu.VMEM)
    return pl.pallas_call(
        functools.partial(kernel, (groups, shards, cores)),
        out_shape=(
            jax.ShapeDtypeStruct((rows, depth), bf),
            jax.ShapeDtypeStruct((depth, width), bf),
            jax.ShapeDtypeStruct((width, depth), bf),
        ),
        in_specs=[vmem] * 3,
        out_specs=(vmem, vmem, vmem),
        scratch_shapes=[
            pltpu.VMEM((shards * rows, depth), bf),
            pltpu.VMEM((inner * rows, width), bf),
            pltpu.VMEM((shards * rows, depth), bf),
            pltpu.VMEM((max(outer * (inner - 1) * heavy, STEP), depth), bf),
            pltpu.VMEM(((outer + 1) * front, depth), bf),
            pltpu.VMEM((max((inner - 1) * light, STEP), depth), bf),
            pltpu.VMEM((max(light, STEP), depth), jnp.float32),
            dma((nseg,)), dma((groups, shards)),
            dma((groups, groups, shards)), dma((groups, groups, shards)),
            dma((groups, groups, cores)), dma((groups, groups)),
            dma((groups,)), dma((groups,)),
            dma((cores, groups)), dma((cores, groups)),
            dma((2 * outer, 3)), dma((outer, 3)),
            dma((inner,)), dma((inner,)),
            dma((outer, inner, 2)), dma((outer, inner, 2)),
            dma((outer, inner, tiles)), dma((outer, inner, tiles)),
            dma((outer, tiles)), dma((outer + 1, tiles)),
            dma((inner, tiles)), dma((inner, tiles)),
            dma((groups, groups, cores, shards)), dma((groups, groups, shards)),
            dma((2,)),
        ],
        compiler_params=pltpu.CompilerParams(
            collective_id=0, has_side_effects=True, vmem_limit_bytes=40 * 1024 * 1024
        ),
        name="serve",
    )(normed, up, down)


def solution(mesh):
    return jax.shard_map(
        body,
        mesh=mesh,
        in_specs=(
            P(("gr", "fs", "tp"), None),
            P(("gr", "fs")),
            P(("gr", "fs"), "tp"),
            P(("gr", "fs"), "tp"),
        ),
        out_specs=(P(("gr", "fs", "tp"), None), P(None, "fs"), P("fs", None)),
        check_vma=False,
    )
```

```python
import functools

import jax
import jax.numpy as jnp
from jax import lax
from jax.experimental import pallas as pl
from jax.experimental.pallas import tpu as pltpu
from jax.sharding import PartitionSpec as P

MESH = pl.DeviceIdType.MESH
TILE = 512
STEP = 16
LAG = 2


def inner_size(shards):
    return max(d for d in range(1, shards + 1) if shards % d == 0 and d * d <= shards)


def heavy_rows(rows, inner):
    return rows if inner == 1 else max(STEP, rows * 3 // 4 // STEP * STEP)


def kernel(sizes, tokens, gain, up_in, down_in, served, su, sd, tok, hid, part, got, far, lit, rest,
           raw, scale, wide_up, wide_down, up, *sems):
    groups, shards, cores = sizes
    inner = inner_size(shards)
    outer = shards // inner
    (up_send, up_recv, gu_send, gu_recv, tu_send, tu_recv, gd_send, gd_recv,
     td_send, td_recv, hop_send, hop_recv, light_send, light_recv, heavy_send, heavy_recv,
     near_send, near_recv, far_send, far_recv, lit_send, lit_recv, ou_send, ou_recv, load, load_up, ou_down_send, ou_down_recv) = sems
    g, f, t = lax.axis_index("gr"), lax.axis_index("fs"), lax.axis_index("tp")
    z, y = f // inner, lax.rem(f, inner)
    rows, depth = raw.shape
    own_rows = up.shape[0]
    segment, dcols = wide_down.shape
    nseg = up.shape[1] // segment
    group_rows = shards * own_rows
    width = su.shape[1]
    heavy = heavy_rows(rows, inner)
    light = rows - heavy
    front = rows + (inner - 1) * light
    stack = inner * rows
    half = rows // 2
    tile = min(TILE, dcols)
    tiles = depth // tile
    cuts = dcols // tile
    low, high = z > 0, z < outer - 1
    middle, end = low & high, jnp.logical_not(low & high)
    near_low = 2 * z < outer - 1
    inward = jnp.where(near_low, 1, -1)

    def to(axis, me, size, step):
        return {axis: lax.rem(me + step, size)}

    def rdma(src, dst, send, recv, device):
        return pltpu.make_async_remote_copy(
            src_ref=src, dst_ref=dst, send_sem=send, recv_sem=recv,
            device_id=device, device_id_type=MESH,
        )

    def back(i):
        return {"fs": z * inner + lax.rem(y + inner - i, inner)}

    def ahead(i):
        return {"fs": z * inner + lax.rem(y + i, inner)}

    def beside(step):
        return {"fs": (z + step) * inner + y}

    def span(ref, start, count, n=None):
        at = pl.ds(start if isinstance(start, int) else pl.multiple_of(start, STEP), count)
        if n is None:
            return ref.at[at]
        return ref.at[at, pl.ds(n * tile if isinstance(n, int) else pl.multiple_of(n * tile, tile), tile)]

    peers = [to("fs", f, shards, k) for k in range(1, shards)]
    peers += [to("gr", g, groups, k) for k in range(1, groups)]
    peers += [to("tp", t, cores, k) for k in range(1, cores)]
    def up_block(group, shard, sg):
        row = pl.multiple_of((group * shards + shard) * own_rows, own_rows)
        return su.at[pl.ds(row, own_rows), pl.ds(pl.multiple_of(sg * segment, segment), segment)]

    def up_group(group, sg):
        row = pl.multiple_of(group * group_rows, group_rows)
        return su.at[pl.ds(row, group_rows), pl.ds(sg * segment, segment)]

    def down_block(group, core):
        row = pl.multiple_of(group * segment, segment)
        return sd.at[pl.ds(row, segment), pl.ds(pl.multiple_of(core * dcols, dcols), dcols)]

    def down_piece(group, core, q):
        row = pl.multiple_of(group * segment, segment)
        return sd.at[pl.ds(row, segment), pl.ds(pl.multiple_of(core * dcols + q * tile, tile), tile)]

    def owner(sg):
        return (sg * shards + f) // nseg

    sends = []

    def begin(copy):
        copy.start()
        sends.append(copy)

    def listed(j, away):
        r, i = j // inner, lax.rem(j, inner)
        rows_z = [z] + [jnp.where(middle, z + a * inward, z + b * inward)
                        for a, b in zip(away, (1, 2, 3))] if outer == 4 else [
                            lax.rem(z + d, outer) for d in range(outer)]
        at = rows_z[0]
        for d in range(1, outer):
            at = jnp.where(r == d, rows_z[d], at)
        return at * inner + lax.rem(y + i, inner)

    loads = [pltpu.make_async_copy(down_in, wide_down, load.at[0]),
             pltpu.make_async_copy(gain, scale, load.at[1]),
             pltpu.make_async_copy(tokens, raw, load.at[2])]

    def load_segment(i):
        cols = pl.ds(pl.multiple_of(i * segment, segment), segment)
        return pltpu.make_async_copy(up_in.at[:, cols], wide_up.at[:, cols], load_up.at[i])

    def target(j):
        return listed(nseg - 1 - j, (-1, 1, 2)) if nseg == shards else lax.rem(f + j, nseg)

    def start_load(j, carry):
        load_segment(target(j)).start()
        return carry

    for copy in loads:
        copy.start()
    lax.fori_loop(0, nseg, start_load, 0)

    barrier = pltpu.get_barrier_semaphore()
    for peer in peers:
        pl.semaphore_signal(barrier, inc=1, device_id=peer, device_id_type=MESH)

    loads[0].wait()

    def round_down(r, carry):
        row = pl.multiple_of(r * STEP, STEP)
        sd[pl.ds(pl.multiple_of(g * segment + row, STEP), STEP), pl.ds(pl.multiple_of(t * dcols, dcols), dcols)] = (
            wide_down[pl.ds(row, STEP), :].astype(jnp.bfloat16))
        return carry

    lax.fori_loop(0, segment // STEP, round_down, 0)
    loads[2].wait()

    def norm(r, carry):
        at = pl.ds(pl.multiple_of(r * STEP, STEP), STEP)
        value = raw[at, :].astype(jnp.float32)
        inverse = lax.rsqrt(jnp.mean(value * value, axis=1, keepdims=True) + 1e-06)
        tok[at, :] = (value * inverse).astype(jnp.bfloat16)
        return carry

    lax.fori_loop(0, rows // STEP, norm, 0)

    loads[1].wait()
    shape = (own_rows, own_rows)
    diagonal = lax.broadcasted_iota(jnp.int32, shape, 0) == lax.broadcasted_iota(jnp.int32, shape, 1)
    column = jnp.sum(jnp.where(diagonal, scale[...], 0.0), axis=1, keepdims=True)
    pl.semaphore_wait(barrier, len(peers))

    def down_copy(k, q):
        block = down_piece(g, t, q)
        return rdma(block, block, gd_send.at[k, q], gd_recv.at[k, q], to("gr", g, groups, k))

    def down_sent(q):
        for k in range(1, groups):
            begin(down_copy(k, q))

    early_cuts = max(1, cuts // 2)
    for q in range(early_cuts):
        down_sent(q)

    pieces = [(0, half), (half, rows - half)] + ([(rows, front - rows)] if front > rows else [])

    def apart(distance):
        low_way, high_way = outer - distance, distance
        return jnp.where(near_low, low_way, high_way), jnp.where(near_low, high_way, low_way)

    def hop(o, way, c):
        start, count = pieces[c]
        step = -inward if way else inward
        n = lax.rem(o + step + outer, outer)
        return rdma(span(tok, o * stack + start, count), span(tok, n * stack + start, count),
                    hop_send.at[o, way, c], hop_recv.at[n, c], beside(step))

    parts = (0, 1) if heavy > half else (0,)
    hops = []

    def move(o, way, which, when):
        for c in which:
            if c < len(pieces):
                pl.when(when)(lambda c=c: hop(o, way, c).start())
                hops.append((o, way, c, when))

    def arrive(o, which, when, way=None):
        for c in which:
            if c < len(pieces):
                start, count = pieces[c]

                @pl.when(when)
                def _(c=c, start=start, count=count):
                    block = span(tok, o * stack + start, count)
                    rdma(block, block, hop_send.at[0, 0, c], hop_recv.at[o, c], beside(0 * z + inward)).wait_recv()

                if way is not None:
                    move(o, way, (c,), when)
                if c in parts:
                    @pl.when(when)
                    def _(c=c):
                        for i in range(1, inner):
                            heavy_copy(o, i, c).start()

    def light_copy(i):
        return rdma(span(tok, heavy, light), span(tok, rows + (i - 1) * light, light),
                    light_send.at[i], light_recv.at[i], ahead(i))

    def heavy_copy(n, i, c):
        start = 0 if c == 0 else half
        count = min(half, heavy) if c == 0 else heavy - half
        src = span(tok, n * stack + start, count)
        return rdma(src, span(tok, n * stack + front + (i - 1) * heavy + start, count),
                    heavy_send.at[n, i, c], heavy_recv.at[n, i, c], ahead(i))


    def up_copy(i):
        number = t * nseg + i
        shard, sg = lax.rem(number, shards), number // shards
        step = lax.rem(shard - f + shards, shards)
        src = up.at[:, pl.ds(pl.multiple_of(i * segment, segment), segment)]
        remote = rdma(src, up_block(g, f, sg), up_send.at[i], up_recv.at[sg, step], {"fs": shard})
        return shard == f, sg, remote

    def start_up(j, carry):
        i = target(j)
        mine, sg, remote = up_copy(i)
        load_segment(i).wait()
        cols = pl.ds(pl.multiple_of(i * segment, segment), segment)
        value = (wide_up[:, cols] * column).astype(jnp.bfloat16)
        up[:, cols] = value

        @pl.when(mine)
        def _():
            row = pl.multiple_of((g * shards + f) * own_rows, own_rows)
            su[pl.ds(row, own_rows), pl.ds(pl.multiple_of(sg * segment, segment), segment)] = value

        pl.when(jnp.logical_not(mine))(remote.start)
        return carry

    zero = z * 0
    in_one, out_one = apart(1)
    if outer > 1:
        move(zero, 0, (0,), z >= 0)
        move(zero, 1, (0,), middle)
    lax.fori_loop(0, nseg, start_up, 0)
    if light:
        for i in range(1, inner):
            begin(light_copy(i))
    if outer > 1:
        move(zero, 0, (1,), z >= 0)
        move(zero, 1, (1,), middle)
    for c in parts:
        for i in range(1, inner):
            begin(heavy_copy(0, i, c))
    for k in range(1, cores):
        block = down_block(g, t)
        begin(rdma(block, block, ou_down_send.at[k], ou_down_recv.at[k], to("tp", t, cores, k)))

    def forward(first, last):
        def of_segment(sg):
            def arrived(j, carry):
                shard = listed(j, (2, -1, 1))
                k = lax.rem(f - shard + shards, shards)
                block = up_block(g, shard, sg)

                @pl.when(k > 0)
                def _():
                    rdma(block, block, up_send.at[0], up_recv.at[sg, k], {"fs": shard}).wait_recv()

                for d in range(1, groups):
                    rdma(block, block, gu_send.at[sg, d, k], gu_recv.at[sg, d, k],
                         to("gr", g, groups, d)).start()
                return carry

            lax.fori_loop(first, last, arrived, 0)
            if last == shards:
                whole = up_group(g, sg)
                for c in range(1, cores):
                    rdma(whole, whole, tu_send.at[sg, 0, c], tu_recv.at[sg, 0], to("tp", t, cores, c)).start()

        for sg in range(groups):
            pl.when(owner(sg) == t)(lambda sg=sg: of_segment(sg))

    forward(0, inner)
    if light:
        for i in range(1, inner):
            light_copy(i).wait_recv()
        if outer > 1:
            move(zero, 0, (2,), z >= 0)
    if outer == 4:
        pl.when(end)(lambda: forward(inner, 2 * inner))
        in_two, in_three = apart(2)[0], apart(3)[0]
        arrive(out_one, (0,), middle, 0)
        arrive(in_one, (0,), middle, 1)
        arrive(in_one, (0,), end)
    if outer == 4:
        pl.when(middle)(lambda: forward(inner, 2 * inner))
    forward(2 * inner if outer == 4 else inner, shards)

    if outer == 4:
        order = [jnp.where(middle, a, b) for a, b in
                 ((in_one, in_two), (out_one, in_three), (in_two, in_one), (zero, zero))]
        arrive(out_one, (1, 2), middle, 0)
        arrive(in_one, (1,), middle, 1)
        arrive(order[0], (2,), middle, 1)
        arrive(in_one, (1,), end)
        arrive(in_two, (0,), end)
        for q in range(early_cuts, cuts):
            down_sent(q)
        arrive(in_two, (1,), end)

    def down_on(q):
        for k in range(1, groups):
            source = lax.rem(g + groups - k, groups)
            block = down_piece(source, t, q)
            rdma(block, block, gd_send.at[k, q], gd_recv.at[k, q], {"gr": source}).wait_recv()
            for c in range(1, cores):
                begin(rdma(block, block, td_send.at[c, k, q], td_recv.at[c, k, q], to("tp", t, cores, c)))

    def down_here(q):
        for c in range(1, cores):
            core = lax.rem(t + cores - c, cores)
            for k in range(1, groups):
                block = down_piece(lax.rem(g + groups - k, groups), core, q)
                rdma(block, block, td_send.at[c, k, q], td_recv.at[c, k, q], {"tp": core}).wait_recv()

    for q in range(early_cuts):
        down_on(q)

    for sg in range(groups):
        def relay(sg=sg):
            for d in range(1, groups):
                source = lax.rem(g + groups - d, groups)

                def arrived(j, carry):
                    shard = listed(j, (2, -1, 1))
                    k = lax.rem(f - shard + shards, shards)
                    block = up_block(source, shard, sg)
                    rdma(block, block, gu_send.at[sg, d, k], gu_recv.at[sg, d, k], {"gr": source}).wait()
                    for c in range(1, cores):
                        rdma(block, block, ou_send.at[sg, d, c, k], ou_recv.at[sg, d, k],
                             to("tp", t, cores, c)).start()
                    return carry

                lax.fori_loop(0, shards, arrived, 0)

        pl.when(owner(sg) == t)(relay)

    for c in range(1, cores):
        core = lax.rem(t + cores - c, cores)
        block = down_block(g, core)
        rdma(block, block, ou_down_send.at[c], ou_down_recv.at[c], {"tp": core}).wait_recv()
    for sg in range(groups):
        def take(sg=sg):
            whole = up_group(g, sg)
            rdma(whole, whole, tu_send.at[sg, 0, 1], tu_recv.at[sg, 0], {"tp": owner(sg)}).wait_recv()
            for d in range(1, groups):
                def taken(k, carry):
                    block = up_block(lax.rem(g + groups - d, groups), lax.rem(f + shards - k, shards), sg)
                    rdma(block, block, tu_send.at[sg, 0, 1], ou_recv.at[sg, d, k],
                         {"tp": owner(sg)}).wait_recv()
                    return carry

                lax.fori_loop(0, shards, taken, 0)

        pl.when(owner(sg) != t)(take)

    def near_copy(o, i, n):
        return rdma(span(part, o * stack + front + (i - 1) * heavy, heavy, n),
                    span(got, (o * (inner - 1) + i - 1) * heavy, heavy, n),
                    near_send.at[o, i, n], near_recv.at[o, i, n], back(i))

    def far_copy(o, n):
        right = o > z
        step = jnp.where(right, 1, -1)
        last = jnp.where(right, o == outer - 1, o == 1)
        slot = jnp.where(last, jnp.where(right, 0, outer), o + step)
        return rdma(span(part, o * stack, front, n), span(far, slot * front, front, n),
                    far_send.at[o, n], far_recv.at[slot, n], beside(step))

    def far_arrived(slot, step, n):
        block = span(far, slot * front, front, n)
        rdma(block, block, far_send.at[0, 0], far_recv.at[slot, n], beside(step)).wait_recv()

    def clear(slot):
        def zero(r, carry):
            far[pl.ds(pl.multiple_of(slot * front + r * STEP, STEP), STEP), :] = jnp.zeros((STEP, depth), jnp.bfloat16)
            return carry

        lax.fori_loop(0, front // STEP, zero, 0)

    def passes(o):
        right = o > z
        return (right & low) | (jnp.logical_not(right) & high)

    pl.when(jnp.logical_not(low))(lambda: clear(0))
    pl.when(jnp.logical_not(high))(lambda: clear(outer))

    def tile_of(s):
        return lax.rem(s, cores) * cuts + s // cores

    def hide(o):
        for i in range(1, inner):
            for c in parts:
                start = 0 if c == 0 else half
                count = min(half, heavy) if c == 0 else heavy - half
                block = span(tok, o * stack + front + (i - 1) * heavy + start, count)
                rdma(block, block, heavy_send.at[o, i, c], heavy_recv.at[o, i, c], back(i)).wait_recv()
        both = pl.ds(pl.multiple_of(o * stack, stack), stack)

        def first(n, carry):
            cols = pl.ds(pl.multiple_of(n * TILE, TILE), TILE)
            product = jnp.dot(tok[both, :], su[:, cols], preferred_element_type=jnp.float32)
            product = jnp.maximum(product, 0.0)
            hid[:, cols] = (product * product).astype(jnp.bfloat16)
            return carry

        lax.fori_loop(0, width // TILE, first, 0)

    def project(o, start, stop):
        both = pl.ds(pl.multiple_of(o * stack, stack), stack)

        def second(s, carry):
            n = tile_of(s)
            cols = pl.ds(pl.multiple_of(n * tile, tile), tile)
            product = jnp.dot(hid[...], sd[:, cols], preferred_element_type=jnp.float32)
            part[both, cols] = product.astype(jnp.bfloat16)
            for i in range(1, inner):
                near_copy(o, i, n).start()
            return carry

        lax.fori_loop(start, stop, second, 0)

    def compute(o):
        hide(o)
        project(o, 0, tiles)

    def gather(o, n):
        for i in range(1, inner):
            near_copy(o, i, n).wait()

    def cells(start, n):
        return pl.ds(pl.multiple_of(start, STEP), STEP), pl.ds(pl.multiple_of(n * tile, tile), tile)

    def value_at(o, r, n, ends, spread):
        value = part[cells(o * stack + r * STEP, n)].astype(jnp.float32)
        if spread:
            for i in range(1, inner):
                value += got[cells((o * (inner - 1) + i - 1) * heavy + r * STEP, n)].astype(jnp.float32)
        for end in ends:
            value += far[cells(end * front + r * STEP, n)].astype(jnp.float32)
        return value

    def add_tile(o, n):
        gather(o, n)

        def sums(ends):
            def chunk(spread, r, carry):
                value = value_at(o, r, n, ends, spread)
                part[cells(o * stack + r * STEP, n)] = value.astype(jnp.bfloat16)
                return carry

            lax.fori_loop(0, heavy // STEP, functools.partial(chunk, True), 0)
            if ends:
                lax.fori_loop(heavy // STEP, front // STEP, functools.partial(chunk, False), 0)

        @pl.when(passes(o))
        def _():
            far_arrived(o, jnp.where(o > z, -1, 1), n)
            sums((o,))

        pl.when(jnp.logical_not(passes(o)))(lambda: sums(()))
        far_copy(o, n).start()

    def add(first, then, start, stop):
        lag = 0 if then is None else LAG

        def tile_sums(s, carry):
            pl.when(s < stop)(lambda: add_tile(first, tile_of(s)))
            if then is not None:
                pl.when(middle & (s >= start + lag))(lambda: add_tile(then, tile_of(s - lag)))
            return carry

        lax.fori_loop(start, stop + lag, tile_sums, 0)

    ready = early_cuts * cores
    if outer == 4:
        for q in range(early_cuts):
            down_here(q)
        arrive(order[0], (2,), end)
        arrive(in_two, (0,), middle, 1)
        hide(order[0])
        project(order[0], 0, ready)
        arrive(in_three, (0,), end)
        pl.when(end)(lambda: add(order[0], None, 0, ready))
        arrive(in_two, (1, 2), middle, 1)
        move(zero, 1, (2,), middle)
        for q in range(early_cuts, cuts):
            down_on(q)
        for q in range(early_cuts, cuts):
            down_here(q)
        project(order[0], ready, tiles)
        arrive(in_three, (1,), end)
        pl.when(end)(lambda: add(order[0], None, ready, tiles))
        arrive(in_three, (2,), end)
        compute(order[1])

        @pl.when(middle)
        def _():
            compute(order[2])
            compute(order[3])
            add(order[0], None, 0, tiles)

        arrive(in_one, (2,), end)
        pl.when(end)(lambda: compute(order[2]))
        add(jnp.where(middle, in_two, in_three), out_one, 0, tiles)

        @pl.when(end)
        def _():
            compute(order[3])
            add(order[2], None, 0, tiles)

    else:
        raise NotImplementedError("rows along z")

    def lit_copy(i, n):
        return rdma(span(part, rows + (i - 1) * light, light, n), span(lit, (i - 1) * light, light, n),
                    lit_send.at[i, n], lit_recv.at[i, n], back(i))

    def total(s, carry):
        n = tile_of(s)
        gather(0, n)
        pl.when(low)(lambda: far_arrived(0, -1, n))
        pl.when(high)(lambda: far_arrived(outer, 1, n))
        ends = (0, outer)

        def others(r, carry):
            part[cells(r * STEP, n)] = value_at(0, r, n, ends, False).astype(jnp.bfloat16)
            return carry

        def half_done(r, carry):
            rest[cells((r * STEP - heavy), n)] = value_at(0, r, n, ends, False)
            return carry

        def done(r, carry):
            served[cells(r * STEP, n)] = value_at(0, r, n, ends, True).astype(jnp.bfloat16)
            return carry

        if light:
            lax.fori_loop(rows // STEP, front // STEP, others, 0)
            for i in range(1, inner):
                lit_copy(i, n).start()
            lax.fori_loop(heavy // STEP, rows // STEP, half_done, 0)
        lax.fori_loop(0, heavy // STEP, done, 0)
        return carry

    lax.fori_loop(0, tiles, total, 0)

    if light:
        def finish(s, carry):
            n = tile_of(s)

            for i in range(1, inner):
                lit_copy(i, n).wait()

            def chunk(r, carry):
                value = rest[cells(r * STEP, n)]
                for i in range(1, inner):
                    value += lit[cells((i - 1) * light + r * STEP, n)].astype(jnp.float32)
                served[cells(heavy + r * STEP, n)] = value.astype(jnp.bfloat16)
                return carry

            lax.fori_loop(0, light // STEP, chunk, 0)
            return carry

        lax.fori_loop(0, tiles, finish, 0)

    for o, way, c, when in hops:
        pl.when(when)(lambda o=o, way=way, c=c: hop(o, way, c).wait_send())
    for n in range(1, outer):
        for c in parts:
            for i in range(1, inner):
                heavy_copy(n, i, c).wait_send()

        def gone(m, carry, n=n):
            far_copy(n, m).wait_send()
            return carry

        lax.fori_loop(0, tiles, gone, 0)
    for copy in sends:
        copy.wait_send()

    def end_up(j, carry):
        mine, sg, remote = up_copy(j)
        pl.when(jnp.logical_not(mine))(remote.wait_send)
        return carry

    lax.fori_loop(0, nseg, end_up, 0)
    for sg in range(groups):
        def end(sg=sg):
            whole = up_group(g, sg)
            for c in range(1, cores):
                rdma(whole, whole, tu_send.at[sg, 0, c], tu_recv.at[sg, 0],
                     to("tp", t, cores, c)).wait_send()
            for d in range(1, groups):
                def left(k, carry):
                    block = up_block(lax.rem(g + groups - d, groups), lax.rem(f + shards - k, shards), sg)
                    for c in range(1, cores):
                        rdma(block, block, ou_send.at[sg, d, c, k], ou_recv.at[sg, d, k],
                             to("tp", t, cores, c)).wait_send()
                    return carry

                lax.fori_loop(0, shards, left, 0)

        pl.when(owner(sg) == t)(end)


def body(tokens, norm_gain, up_weight, down_weight):
    groups, shards, cores = (lax.axis_size(a) for a in ("gr", "fs", "tp"))
    segment = down_weight.shape[0]
    rows, depth = tokens.shape
    inner = inner_size(shards)
    outer = shards // inner
    heavy = heavy_rows(rows, inner)
    light = rows - heavy
    front = rows + (inner - 1) * light
    own_rows, columns = up_weight.shape
    nseg = columns // segment
    width = groups * segment
    dcols = down_weight.shape[1]
    tile = min(TILE, dcols)
    tiles = depth // tile
    cuts = dcols // tile
    bf = jnp.bfloat16
    dma = pltpu.SemaphoreType.DMA
    vmem = pl.BlockSpec(memory_space=pltpu.VMEM)
    return pl.pallas_call(
        functools.partial(kernel, (groups, shards, cores)),
        out_shape=(
            jax.ShapeDtypeStruct((rows, depth), bf),
            jax.ShapeDtypeStruct((depth, width), bf),
            jax.ShapeDtypeStruct((width, depth), bf),
        ),
        in_specs=[pl.BlockSpec(memory_space=pltpu.HBM)] * 4,
        out_specs=(vmem, vmem, vmem),
        scratch_shapes=[
            pltpu.VMEM((shards * rows, depth), bf),
            pltpu.VMEM((inner * rows, width), bf),
            pltpu.VMEM((shards * rows, depth), bf),
            pltpu.VMEM((max(outer * (inner - 1) * heavy, STEP), depth), bf),
            pltpu.VMEM(((outer + 1) * front, depth), bf),
            pltpu.VMEM((max((inner - 1) * light, STEP), depth), bf),
            pltpu.VMEM((max(light, STEP), depth), jnp.float32),
            pltpu.VMEM((rows, depth), bf),
            pltpu.VMEM((1, own_rows), jnp.float32),
            pltpu.VMEM((own_rows, columns), jnp.float32),
            pltpu.VMEM((segment, dcols), jnp.float32),
            pltpu.VMEM((own_rows, columns), bf),
            dma((nseg,)), dma((groups, shards)),
            dma((groups, groups, shards)), dma((groups, groups, shards)),
            dma((groups, groups, cores)), dma((groups, groups)),
            dma((groups, cuts)), dma((groups, cuts)),
            dma((cores, groups, cuts)), dma((cores, groups, cuts)),
            dma((outer, 2, 3)), dma((outer, 3)),
            dma((inner,)), dma((inner,)),
            dma((outer, inner, 2)), dma((outer, inner, 2)),
            dma((outer, inner, tiles)), dma((outer, inner, tiles)),
            dma((outer, tiles)), dma((outer + 1, tiles)),
            dma((inner, tiles)), dma((inner, tiles)),
            dma((groups, groups, cores, shards)), dma((groups, groups, shards)),
            dma((3,)), dma((nseg,)), dma((cores,)), dma((cores,)),
        ],
        compiler_params=pltpu.CompilerParams(
            collective_id=0, has_side_effects=True, vmem_limit_bytes=40 * 1024 * 1024
        ),
        name="serve",
    )(*(pltpu.with_memory_space_constraint(a, pltpu.HBM) for a in (tokens, norm_gain[None, :], up_weight, down_weight)))


def solution(mesh):
    return jax.shard_map(
        body,
        mesh=mesh,
        in_specs=(
            P(("gr", "fs", "tp"), None),
            P(("gr", "fs")),
            P(("gr", "fs"), "tp"),
            P(("gr", "fs"), "tp"),
        ),
        out_specs=(P(("gr", "fs", "tp"), None), P(None, "fs"), P("fs", None)),
        check_vma=False,
    )
```

```python
import functools

import jax
import jax.numpy as jnp
from jax import lax
from jax.experimental import pallas as pl
from jax.experimental.pallas import tpu as pltpu
from jax.sharding import PartitionSpec as P

MESH = pl.DeviceIdType.MESH
TILE = 512
STEP = 16
LAG = 1
BEHIND = 2
HEAVY = 6


def inner_size(shards):
    return max(d for d in range(1, shards + 1) if shards % d == 0 and d * d <= shards)


def heavy_rows(rows, inner):
    return rows * HEAVY // 8 // STEP * STEP


def kernel(sizes, tokens, gain, up_in, down_in, served, su, sd, tok, hid, part, got, far, lit, rest,
           raw, scale, wide_up, wide_down, up, *sems):
    groups, shards, cores = sizes
    inner = inner_size(shards)
    outer = shards // inner
    (up_send, up_recv, gu_send, gu_recv, tu_send, tu_recv, gd_send, gd_recv,
     td_send, td_recv, hop_send, hop_recv, light_send, light_recv, heavy_send, heavy_recv,
     near_send, near_recv, far_send, far_recv, lit_send, lit_recv, ou_send, ou_recv, load, load_up, ou_down_send, ou_down_recv) = sems
    g, f, t = lax.axis_index("gr"), lax.axis_index("fs"), lax.axis_index("tp")
    z, y = f // inner, lax.rem(f, inner)
    rows, depth = raw.shape
    own_rows = up.shape[0]
    segment, dcols = wide_down.shape
    nseg = up.shape[1] // segment
    group_rows = shards * own_rows
    width = su.shape[1]
    heavy = heavy_rows(rows, inner)
    light = rows - heavy
    front = rows + (inner - 1) * light
    stack = inner * rows
    half = rows // 2
    tile = min(TILE, dcols)
    tiles = depth // tile
    cuts = dcols // tile
    low, high = z > 0, z < outer - 1
    middle, end = low & high, jnp.logical_not(low & high)
    near_low = 2 * z < outer - 1
    inward = jnp.where(near_low, 1, -1)

    def to(axis, me, size, step):
        return {axis: lax.rem(me + step, size)}

    def rdma(src, dst, send, recv, device):
        return pltpu.make_async_remote_copy(
            src_ref=src, dst_ref=dst, send_sem=send, recv_sem=recv,
            device_id=device, device_id_type=MESH,
        )

    def back(i):
        return {"fs": z * inner + lax.rem(y + inner - i, inner)}

    def ahead(i):
        return {"fs": z * inner + lax.rem(y + i, inner)}

    def beside(step):
        return {"fs": (z + step) * inner + y}

    def span(ref, start, count, n=None):
        at = pl.ds(start if isinstance(start, int) else pl.multiple_of(start, STEP), count)
        if n is None:
            return ref.at[at]
        return ref.at[at, pl.ds(n * tile if isinstance(n, int) else pl.multiple_of(n * tile, tile), tile)]

    peers = [to("fs", f, shards, k) for k in range(1, shards)]
    peers += [to("gr", g, groups, k) for k in range(1, groups)]
    peers += [to("tp", t, cores, k) for k in range(1, cores)]
    def up_block(group, shard, sg):
        row = pl.multiple_of((group * shards + shard) * own_rows, own_rows)
        return su.at[pl.ds(row, own_rows), pl.ds(pl.multiple_of(sg * segment, segment), segment)]

    def up_group(group, sg):
        row = pl.multiple_of(group * group_rows, group_rows)
        return su.at[pl.ds(row, group_rows), pl.ds(sg * segment, segment)]

    def down_block(group, core):
        row = pl.multiple_of(group * segment, segment)
        return sd.at[pl.ds(row, segment), pl.ds(pl.multiple_of(core * dcols, dcols), dcols)]

    def down_piece(group, core, q):
        row = pl.multiple_of(group * segment, segment)
        return sd.at[pl.ds(row, segment), pl.ds(pl.multiple_of(core * dcols + q * tile, tile), tile)]

    def owner(sg):
        return (sg * shards + f) // nseg

    sends = []

    def begin(copy):
        copy.start()
        sends.append(copy)

    def listed(j, middle_rows, end_rows):
        r, i = j // inner, lax.rem(j, inner)
        if outer == 4:
            rows_z = [jnp.where(middle, z + a * inward, z + b * inward) for a, b in zip(middle_rows, end_rows)]
        else:
            rows_z = [lax.rem(z + d, outer) for d in range(outer)]
        at = rows_z[0]
        for d in range(1, outer):
            at = jnp.where(r == d, rows_z[d], at)
        return at * inner + lax.rem(y + i, inner)

    loads = [pltpu.make_async_copy(down_in, wide_down, load.at[0]),
             pltpu.make_async_copy(gain, scale, load.at[1]),
             pltpu.make_async_copy(tokens, raw, load.at[2])]

    def load_segment(i):
        cols = pl.ds(pl.multiple_of(i * segment, segment), segment)
        return pltpu.make_async_copy(up_in.at[:, cols], wide_up.at[:, cols], load_up.at[i])

    def target(j):
        return listed(j, (2, -1, 0, 1), (3, 2, 0, 1)) if nseg == shards else lax.rem(f + j, nseg)

    def start_load(j, carry):
        load_segment(target(j)).start()
        return carry

    for copy in loads:
        copy.start()
    lax.fori_loop(0, nseg, start_load, 0)

    barrier = pltpu.get_barrier_semaphore()
    for peer in peers:
        pl.semaphore_signal(barrier, inc=1, device_id=peer, device_id_type=MESH)

    loads[0].wait()

    def round_down(r, carry):
        row = pl.multiple_of(r * STEP, STEP)
        sd[pl.ds(pl.multiple_of(g * segment + row, STEP), STEP), pl.ds(pl.multiple_of(t * dcols, dcols), dcols)] = (
            wide_down[pl.ds(row, STEP), :].astype(jnp.bfloat16))
        return carry

    lax.fori_loop(0, segment // STEP, round_down, 0)
    loads[2].wait()

    def norm(r, carry):
        at = pl.ds(pl.multiple_of(r * STEP, STEP), STEP)
        value = raw[at, :].astype(jnp.float32)
        inverse = lax.rsqrt(jnp.mean(value * value, axis=1, keepdims=True) + 1e-06)
        tok[at, :] = (value * inverse).astype(jnp.bfloat16)
        return carry

    lax.fori_loop(0, rows // STEP, norm, 0)

    loads[1].wait()
    shape = (own_rows, own_rows)
    diagonal = lax.broadcasted_iota(jnp.int32, shape, 0) == lax.broadcasted_iota(jnp.int32, shape, 1)
    column = jnp.sum(jnp.where(diagonal, scale[...], 0.0), axis=1, keepdims=True)
    pl.semaphore_wait(barrier, len(peers))

    def down_copy(k, q):
        block = down_piece(g, t, q)
        return rdma(block, block, gd_send.at[k, q], gd_recv.at[k, q], to("gr", g, groups, k))

    def down_sent(q):
        for k in range(1, groups):
            begin(down_copy(k, q))

    early_cuts = max(1, cuts // 2)
    for q in range(early_cuts):
        down_sent(q)

    pieces = [(0, half), (half, heavy - half), (heavy, front - heavy)]

    def apart(distance):
        low_way, high_way = outer - distance, distance
        return jnp.where(near_low, low_way, high_way), jnp.where(near_low, high_way, low_way)

    def hop(o, way, c):
        start, count = pieces[c]
        step = -inward if way else inward
        n = lax.rem(o + step + outer, outer)
        return rdma(span(tok, o * stack + start, count), span(tok, n * stack + start, count),
                    hop_send.at[o, way, c], hop_recv.at[n, c], beside(step))

    parts = (0, 1)
    hops = []

    def move(o, way, which, when):
        for c in which:
            if c < len(pieces):
                pl.when(when)(lambda c=c: hop(o, way, c).start())
                hops.append((o, way, c, when))

    def arrive(o, which, when, way=None):
        for c in which:
            if c < len(pieces):
                start, count = pieces[c]

                @pl.when(when)
                def _(c=c, start=start, count=count):
                    block = span(tok, o * stack + start, count)
                    rdma(block, block, hop_send.at[0, 0, c], hop_recv.at[o, c], beside(0 * z + inward)).wait_recv()

                if way is not None:
                    move(o, way, (c,), when)
                if c in parts:
                    @pl.when(when)
                    def _(c=c):
                        for i in range(1, inner):
                            heavy_copy(o, i, c).start()

    def light_copy(i):
        return rdma(span(tok, heavy, light), span(tok, rows + (i - 1) * light, light),
                    light_send.at[i], light_recv.at[i], ahead(i))

    def heavy_copy(n, i, c):
        start = 0 if c == 0 else half
        count = min(half, heavy) if c == 0 else heavy - half
        src = span(tok, n * stack + start, count)
        return rdma(src, span(tok, n * stack + front + (i - 1) * heavy + start, count),
                    heavy_send.at[n, i, c], heavy_recv.at[n, i, c], ahead(i))


    def up_copy(i):
        number = t * nseg + i
        shard, sg = lax.rem(number, shards), number // shards
        step = lax.rem(shard - f + shards, shards)
        src = up.at[:, pl.ds(pl.multiple_of(i * segment, segment), segment)]
        remote = rdma(src, up_block(g, f, sg), up_send.at[i], up_recv.at[sg, step], {"fs": shard})
        return shard == f, sg, remote

    def start_up(j, carry):
        i = target(j)
        mine, sg, remote = up_copy(i)
        load_segment(i).wait()
        cols = pl.ds(pl.multiple_of(i * segment, segment), segment)
        value = (wide_up[:, cols] * column).astype(jnp.bfloat16)
        up[:, cols] = value

        @pl.when(mine)
        def _():
            row = pl.multiple_of((g * shards + f) * own_rows, own_rows)
            su[pl.ds(row, own_rows), pl.ds(pl.multiple_of(sg * segment, segment), segment)] = value

        pl.when(jnp.logical_not(mine))(remote.start)
        return carry

    zero = z * 0
    in_one, out_one = apart(1)
    first_part = inner if nseg == shards else nseg
    last_part = shards - inner if nseg == shards else nseg
    move(zero, 0, (0,), z >= 0)
    if light:
        for i in range(1, inner):
            begin(light_copy(i))
    lax.fori_loop(0, first_part, start_up, 0)
    move(zero, 0, (1,), middle)
    lax.fori_loop(first_part, last_part, start_up, 0)
    move(zero, 1, (0,), middle)
    for c in parts:
        for i in range(1, inner):
            begin(heavy_copy(0, i, c))
    for k in range(1, cores):
        block = down_block(g, t)
        begin(rdma(block, block, ou_down_send.at[k], ou_down_recv.at[k], to("tp", t, cores, k)))

    def down_rest():
        for q in range(early_cuts, cuts):
            for k in range(1, groups):
                down_copy(k, q).start()

    def forward(first, last):
        def of_segment(sg):
            def arrived(j, carry):
                shard = listed(j, (0, 2, -1, 1), (0, 1, 2, 3))
                k = lax.rem(f - shard + shards, shards)
                block = up_block(g, shard, sg)

                @pl.when(k > 0)
                def _():
                    rdma(block, block, up_send.at[0], up_recv.at[sg, k], {"fs": shard}).wait_recv()

                for d in range(1, groups):
                    rdma(block, block, gu_send.at[sg, d, k], gu_recv.at[sg, d, k],
                         to("gr", g, groups, d)).start()
                return carry

            lax.fori_loop(first, last, arrived, 0)
            if last == shards:
                whole = up_group(g, sg)
                for c in range(1, cores):
                    rdma(whole, whole, tu_send.at[sg, 0, c], tu_recv.at[sg, 0], to("tp", t, cores, c)).start()

        for sg in range(groups):
            pl.when(owner(sg) == t)(lambda sg=sg: of_segment(sg))

    forward(0, 1)
    if light:
        for i in range(1, inner):
            light_copy(i).wait_recv()
    move(zero, 0, (2,), middle)
    lax.fori_loop(last_part, nseg, start_up, 0)
    move(zero, 0, (1, 2), end)
    forward(1, inner)
    if outer == 4:
        pl.when(end)(lambda: forward(inner, shards))
        in_two, in_three = apart(2)[0], apart(3)[0]
        arrive(out_one, (0,), middle, 0)
        arrive(in_one, (0,), middle, 1)
        arrive(in_one, (0,), end)
    if outer == 4:
        pl.when(middle)(lambda: forward(inner, 3 * inner))
        pl.when(middle)(down_rest)
    else:
        forward(inner, shards)

    if outer == 4:
        order = [jnp.where(middle, a, b) for a, b in
                 ((in_one, in_two), (in_two, in_three), (out_one, in_one), (zero, zero))]
        arrive(in_one, (1,), middle, 1)
        arrive(order[0], (2,), middle, 1)
        move(zero, 1, (1,), middle)
        arrive(out_one, (1, 2), middle, 0)
        pl.when(middle)(lambda: forward(3 * inner, shards))
        arrive(in_two, (0,), middle, 1)
        arrive(in_two, (0,), end)
        pl.when(end)(down_rest)
        arrive(in_two, (1,), end)

    def down_on(q):
        for k in range(1, groups):
            source = lax.rem(g + groups - k, groups)
            block = down_piece(source, t, q)
            rdma(block, block, gd_send.at[k, q], gd_recv.at[k, q], {"gr": source}).wait_recv()
            for c in range(1, cores):
                begin(rdma(block, block, td_send.at[c, k, q], td_recv.at[c, k, q], to("tp", t, cores, c)))

    def down_here(q):
        for c in range(1, cores):
            core = lax.rem(t + cores - c, cores)
            for k in range(1, groups):
                block = down_piece(lax.rem(g + groups - k, groups), core, q)
                rdma(block, block, td_send.at[c, k, q], td_recv.at[c, k, q], {"tp": core}).wait_recv()

    for q in range(early_cuts):
        down_on(q)

    for sg in range(groups):
        def relay(sg=sg):
            for d in range(1, groups):
                source = lax.rem(g + groups - d, groups)

                def arrived(j, carry):
                    shard = listed(j, (0, 2, -1, 1), (0, 1, 2, 3))
                    k = lax.rem(f - shard + shards, shards)
                    block = up_block(source, shard, sg)
                    rdma(block, block, gu_send.at[sg, d, k], gu_recv.at[sg, d, k], {"gr": source}).wait()
                    for c in range(1, cores):
                        rdma(block, block, ou_send.at[sg, d, c, k], ou_recv.at[sg, d, k],
                             to("tp", t, cores, c)).start()
                    return carry

                lax.fori_loop(0, shards, arrived, 0)

        pl.when(owner(sg) == t)(relay)

    for c in range(1, cores):
        core = lax.rem(t + cores - c, cores)
        block = down_block(g, core)
        rdma(block, block, ou_down_send.at[c], ou_down_recv.at[c], {"tp": core}).wait_recv()
    for sg in range(groups):
        def take(sg=sg):
            whole = up_group(g, sg)
            rdma(whole, whole, tu_send.at[sg, 0, 1], tu_recv.at[sg, 0], {"tp": owner(sg)}).wait_recv()
            for d in range(1, groups):
                def taken(k, carry):
                    block = up_block(lax.rem(g + groups - d, groups), lax.rem(f + shards - k, shards), sg)
                    rdma(block, block, tu_send.at[sg, 0, 1], ou_recv.at[sg, d, k],
                         {"tp": owner(sg)}).wait_recv()
                    return carry

                lax.fori_loop(0, shards, taken, 0)

        pl.when(owner(sg) != t)(take)

    def near_copy(o, i, n):
        return rdma(span(part, o * stack + front + (i - 1) * heavy, heavy, n),
                    span(got, (o * (inner - 1) + i - 1) * heavy, heavy, n),
                    near_send.at[o, i, n], near_recv.at[o, i, n], back(i))

    def far_copy(o, n):
        right = o > z
        step = jnp.where(right, 1, -1)
        last = jnp.where(right, o == outer - 1, o == 1)
        slot = jnp.where(last, jnp.where(right, 0, outer), o + step)
        return rdma(span(part, o * stack, front, n), span(far, slot * front, front, n),
                    far_send.at[o, n], far_recv.at[slot, n], beside(step))

    def far_arrived(slot, step, n):
        block = span(far, slot * front, front, n)
        rdma(block, block, far_send.at[0, 0], far_recv.at[slot, n], beside(step)).wait_recv()

    def clear(slot):
        def zero(r, carry):
            far[pl.ds(pl.multiple_of(slot * front + r * STEP, STEP), STEP), :] = jnp.zeros((STEP, depth), jnp.bfloat16)
            return carry

        lax.fori_loop(0, front // STEP, zero, 0)

    def passes(o):
        right = o > z
        return (right & low) | (jnp.logical_not(right) & high)

    pl.when(jnp.logical_not(low))(lambda: clear(0))
    pl.when(jnp.logical_not(high))(lambda: clear(outer))

    def tile_of(s):
        return lax.rem(s, cores) * cuts + s // cores

    def hide(o):
        for i in range(1, inner):
            for c in parts:
                start = 0 if c == 0 else half
                count = min(half, heavy) if c == 0 else heavy - half
                block = span(tok, o * stack + front + (i - 1) * heavy + start, count)
                rdma(block, block, heavy_send.at[o, i, c], heavy_recv.at[o, i, c], back(i)).wait_recv()
        both = pl.ds(pl.multiple_of(o * stack, stack), stack)

        def first(n, carry):
            cols = pl.ds(pl.multiple_of(n * TILE, TILE), TILE)
            product = jnp.dot(tok[both, :], su[:, cols], preferred_element_type=jnp.float32)
            product = jnp.maximum(product, 0.0)
            hid[:, cols] = (product * product).astype(jnp.bfloat16)
            return carry

        lax.fori_loop(0, width // TILE, first, 0)

    def project(o, start, stop):
        both = pl.ds(pl.multiple_of(o * stack, stack), stack)

        def second(s, carry):
            n = tile_of(s)
            cols = pl.ds(pl.multiple_of(n * tile, tile), tile)
            product = jnp.dot(hid[...], sd[:, cols], preferred_element_type=jnp.float32)
            part[both, cols] = product.astype(jnp.bfloat16)
            for i in range(1, inner):
                near_copy(o, i, n).start()
            return carry

        lax.fori_loop(start, stop, second, 0)

    def compute(o):
        hide(o)
        project(o, 0, tiles)

    def gather(o, n):
        for i in range(1, inner):
            near_copy(o, i, n).wait()

    def cells(start, n):
        return pl.ds(pl.multiple_of(start, STEP), STEP), pl.ds(pl.multiple_of(n * tile, tile), tile)

    def value_at(o, r, n, ends, spread):
        value = part[cells(o * stack + r * STEP, n)].astype(jnp.float32)
        if spread:
            for i in range(1, inner):
                value += got[cells((o * (inner - 1) + i - 1) * heavy + r * STEP, n)].astype(jnp.float32)
        for end in ends:
            value += far[cells(end * front + r * STEP, n)].astype(jnp.float32)
        return value

    def add_tile(o, n):
        gather(o, n)

        def sums(ends):
            def chunk(spread, r, carry):
                value = value_at(o, r, n, ends, spread)
                part[cells(o * stack + r * STEP, n)] = value.astype(jnp.bfloat16)
                return carry

            lax.fori_loop(0, heavy // STEP, functools.partial(chunk, True), 0)
            if ends:
                lax.fori_loop(heavy // STEP, front // STEP, functools.partial(chunk, False), 0)

        @pl.when(passes(o))
        def _():
            far_arrived(o, jnp.where(o > z, -1, 1), n)
            sums((o,))

        pl.when(jnp.logical_not(passes(o)))(lambda: sums(()))
        far_copy(o, n).start()

    def add(first, then, start, stop):
        lag = 0 if then is None else LAG

        def tile_sums(s, carry):
            pl.when(s < stop)(lambda: add_tile(first, tile_of(s)))
            if then is not None:
                pl.when(middle & (s >= start + lag))(lambda: add_tile(then, tile_of(s - lag)))
            return carry

        lax.fori_loop(start, stop + lag, tile_sums, 0)

    def beside_sums(o, later):
        def step(s, carry):
            pl.when(s < tiles)(lambda: add_tile(o, tile_of(s)))
            pl.when(s >= BEHIND)(lambda: project(later, s - BEHIND, s - BEHIND + 1))
            return carry

        lax.fori_loop(0, tiles + BEHIND, step, 0)

    def wait_far():
        def gone(s, carry):
            far_copy(in_three, tile_of(s)).wait_send()
            return carry

        lax.fori_loop(0, tiles - 1, gone, 0)

    ready = early_cuts * cores
    if outer == 4:
        for q in range(early_cuts):
            down_here(q)
        arrive(order[0], (2,), end)
        hide(order[0])
        project(order[0], 0, ready)
        arrive(in_one, (1,), end)
        arrive(in_three, (0,), end)
        arrive(in_two, (1, 2), middle, 1)
        move(zero, 1, (2,), middle)
        for q in range(early_cuts, cuts):
            down_on(q)
        for q in range(early_cuts, cuts):
            down_here(q)
        project(order[0], ready, tiles)
        arrive(in_three, (1,), end)
        pl.when(end)(lambda: add(order[0], None, 0, ready))
        pl.when(end)(lambda: add(order[0], None, ready, tiles))
        arrive(in_three, (2,), end)
        compute(order[1])

        @pl.when(middle)
        def _():
            add(order[0], None, 0, tiles // 2)
            compute(order[2])
            add(order[0], None, tiles // 2, tiles)
            compute(order[3])
            add(in_two, out_one, 0, tiles)

        arrive(in_one, (2,), end)

        @pl.when(end)
        def _():
            hide(order[2])
            beside_sums(in_three, order[2])
            hide(order[3])
            wait_far()
            beside_sums(order[2], order[3])

    else:
        raise NotImplementedError("rows along z")

    def lit_copy(i, n):
        return rdma(span(part, rows + (i - 1) * light, light, n), span(lit, (i - 1) * light, light, n),
                    lit_send.at[i, n], lit_recv.at[i, n], back(i))

    def total(s, carry):
        n = tile_of(s)
        gather(0, n)
        pl.when(low)(lambda: far_arrived(0, -1, n))
        pl.when(high)(lambda: far_arrived(outer, 1, n))
        ends = (0, outer)

        def others(r, carry):
            part[cells(r * STEP, n)] = value_at(0, r, n, ends, False).astype(jnp.bfloat16)
            return carry

        def half_done(r, carry):
            rest[cells((r * STEP - heavy), n)] = value_at(0, r, n, ends, False)
            return carry

        def done(r, carry):
            served[cells(r * STEP, n)] = value_at(0, r, n, ends, True).astype(jnp.bfloat16)
            return carry

        if light:
            lax.fori_loop(rows // STEP, front // STEP, others, 0)
            for i in range(1, inner):
                lit_copy(i, n).start()
            lax.fori_loop(heavy // STEP, rows // STEP, half_done, 0)
        lax.fori_loop(0, heavy // STEP, done, 0)
        return carry

    lax.fori_loop(0, tiles, total, 0)

    if light:
        def finish(s, carry):
            n = tile_of(s)

            for i in range(1, inner):
                lit_copy(i, n).wait()

            def chunk(r, carry):
                value = rest[cells(r * STEP, n)]
                for i in range(1, inner):
                    value += lit[cells((i - 1) * light + r * STEP, n)].astype(jnp.float32)
                served[cells(heavy + r * STEP, n)] = value.astype(jnp.bfloat16)
                return carry

            lax.fori_loop(0, light // STEP, chunk, 0)
            return carry

        lax.fori_loop(0, tiles, finish, 0)

    for o, way, c, when in hops:
        pl.when(when)(lambda o=o, way=way, c=c: hop(o, way, c).wait_send())
    for n in range(1, outer):
        for c in parts:
            for i in range(1, inner):
                heavy_copy(n, i, c).wait_send()

        def gone(m, carry, n=n):
            waited = end & (n == apart(3)[0]) & (m != tile_of(tiles - 1))
            pl.when(jnp.logical_not(waited))(lambda: far_copy(n, m).wait_send())
            return carry

        lax.fori_loop(0, tiles, gone, 0)
    for copy in sends:
        copy.wait_send()
    for q in range(early_cuts, cuts):
        for k in range(1, groups):
            down_copy(k, q).wait_send()

    def end_up(j, carry):
        mine, sg, remote = up_copy(j)
        pl.when(jnp.logical_not(mine))(remote.wait_send)
        return carry

    lax.fori_loop(0, nseg, end_up, 0)
    for sg in range(groups):
        def end(sg=sg):
            whole = up_group(g, sg)
            for c in range(1, cores):
                rdma(whole, whole, tu_send.at[sg, 0, c], tu_recv.at[sg, 0],
                     to("tp", t, cores, c)).wait_send()
            for d in range(1, groups):
                def left(k, carry):
                    block = up_block(lax.rem(g + groups - d, groups), lax.rem(f + shards - k, shards), sg)
                    for c in range(1, cores):
                        rdma(block, block, ou_send.at[sg, d, c, k], ou_recv.at[sg, d, k],
                             to("tp", t, cores, c)).wait_send()
                    return carry

                lax.fori_loop(0, shards, left, 0)

        pl.when(owner(sg) == t)(end)


def body(tokens, norm_gain, up_weight, down_weight):
    groups, shards, cores = (lax.axis_size(a) for a in ("gr", "fs", "tp"))
    segment = down_weight.shape[0]
    rows, depth = tokens.shape
    inner = inner_size(shards)
    outer = shards // inner
    heavy = heavy_rows(rows, inner)
    light = rows - heavy
    front = rows + (inner - 1) * light
    own_rows, columns = up_weight.shape
    nseg = columns // segment
    width = groups * segment
    dcols = down_weight.shape[1]
    tile = min(TILE, dcols)
    tiles = depth // tile
    cuts = dcols // tile
    bf = jnp.bfloat16
    dma = pltpu.SemaphoreType.DMA
    vmem = pl.BlockSpec(memory_space=pltpu.VMEM)
    return pl.pallas_call(
        functools.partial(kernel, (groups, shards, cores)),
        out_shape=(
            jax.ShapeDtypeStruct((rows, depth), bf),
            jax.ShapeDtypeStruct((depth, width), bf),
            jax.ShapeDtypeStruct((width, depth), bf),
        ),
        in_specs=[pl.BlockSpec(memory_space=pltpu.HBM)] * 4,
        out_specs=(vmem, vmem, vmem),
        scratch_shapes=[
            pltpu.VMEM((shards * rows, depth), bf),
            pltpu.VMEM((inner * rows, width), bf),
            pltpu.VMEM((shards * rows, depth), bf),
            pltpu.VMEM((max(outer * (inner - 1) * heavy, STEP), depth), bf),
            pltpu.VMEM(((outer + 1) * front, depth), bf),
            pltpu.VMEM((max((inner - 1) * light, STEP), depth), bf),
            pltpu.VMEM((max(light, STEP), depth), jnp.float32),
            pltpu.VMEM((rows, depth), bf),
            pltpu.VMEM((1, own_rows), jnp.float32),
            pltpu.VMEM((own_rows, columns), jnp.float32),
            pltpu.VMEM((segment, dcols), jnp.float32),
            pltpu.VMEM((own_rows, columns), bf),
            dma((nseg,)), dma((groups, shards)),
            dma((groups, groups, shards)), dma((groups, groups, shards)),
            dma((groups, groups, cores)), dma((groups, groups)),
            dma((groups, cuts)), dma((groups, cuts)),
            dma((cores, groups, cuts)), dma((cores, groups, cuts)),
            dma((outer, 2, 3)), dma((outer, 3)),
            dma((inner,)), dma((inner,)),
            dma((outer, inner, 2)), dma((outer, inner, 2)),
            dma((outer, inner, tiles)), dma((outer, inner, tiles)),
            dma((outer, tiles)), dma((outer + 1, tiles)),
            dma((inner, tiles)), dma((inner, tiles)),
            dma((groups, groups, cores, shards)), dma((groups, groups, shards)),
            dma((3,)), dma((nseg,)), dma((cores,)), dma((cores,)),
        ],
        compiler_params=pltpu.CompilerParams(
            collective_id=0, has_side_effects=True, vmem_limit_bytes=40 * 1024 * 1024
        ),
        name="serve",
    )(*(pltpu.with_memory_space_constraint(a, pltpu.HBM) for a in (tokens, norm_gain[None, :], up_weight, down_weight)))


def solution(mesh):
    return jax.shard_map(
        body,
        mesh=mesh,
        in_specs=(
            P(("gr", "fs", "tp"), None),
            P(("gr", "fs")),
            P(("gr", "fs"), "tp"),
            P(("gr", "fs"), "tp"),
        ),
        out_specs=(P(("gr", "fs", "tp"), None), P(None, "fs"), P("fs", None)),
        check_vma=False,
    )
```

```python
import functools

import jax
import jax.numpy as jnp
from jax import lax
from jax.experimental import pallas as pl
from jax.experimental.pallas import tpu as pltpu
from jax.sharding import PartitionSpec as P

MESH = pl.DeviceIdType.MESH
TILE = 512
STEP = 16
LAG = 1
BEHIND = 2
HEAVY = 6
CUTS = 2


def inner_size(shards):
    return max(d for d in range(1, shards + 1) if shards % d == 0 and d * d <= shards)


def heavy_rows(rows, inner):
    return rows * HEAVY // 8 // STEP * STEP


def kernel(sizes, tokens, gain, up_in, down_in, served, su, sd, tok, hid, part, got, far, lit, rest,
           raw, scale, wide_up, wide_down, up, *sems):
    groups, shards, cores = sizes
    inner = inner_size(shards)
    outer = shards // inner
    (up_send, up_recv, gu_send, gu_recv, tu_send, tu_recv, gd_send, gd_recv,
     td_send, td_recv, hop_send, hop_recv, light_send, light_recv, heavy_send, heavy_recv,
     near_send, near_recv, far_send, far_recv, lit_send, lit_recv, ou_send, ou_recv, load, load_up, ou_down_send, ou_down_recv) = sems
    g, f, t = lax.axis_index("gr"), lax.axis_index("fs"), lax.axis_index("tp")
    z, y = f // inner, lax.rem(f, inner)
    rows, depth = raw.shape
    own_rows = up.shape[0]
    segment, dcols = wide_down.shape
    nseg = up.shape[1] // segment
    group_rows = shards * own_rows
    width = su.shape[1]
    heavy = heavy_rows(rows, inner)
    light = rows - heavy
    front = rows + (inner - 1) * light
    stack = inner * rows
    half = rows // 2
    tile = min(TILE, dcols)
    tiles = depth // tile
    cuts = dcols // tile
    low, high = z > 0, z < outer - 1
    middle, end = low & high, jnp.logical_not(low & high)
    near_low = 2 * z < outer - 1
    inward = jnp.where(near_low, 1, -1)

    def to(axis, me, size, step):
        return {axis: lax.rem(me + step, size)}

    def rdma(src, dst, send, recv, device):
        return pltpu.make_async_remote_copy(
            src_ref=src, dst_ref=dst, send_sem=send, recv_sem=recv,
            device_id=device, device_id_type=MESH,
        )

    def back(i):
        return {"fs": z * inner + lax.rem(y + inner - i, inner)}

    def ahead(i):
        return {"fs": z * inner + lax.rem(y + i, inner)}

    def beside(step):
        return {"fs": (z + step) * inner + y}

    def span(ref, start, count, n=None):
        at = pl.ds(start if isinstance(start, int) else pl.multiple_of(start, STEP), count)
        if n is None:
            return ref.at[at]
        return ref.at[at, pl.ds(n * tile if isinstance(n, int) else pl.multiple_of(n * tile, tile), tile)]

    peers = [to("fs", f, shards, k) for k in range(1, shards)]
    peers += [to("gr", g, groups, k) for k in range(1, groups)]
    peers += [to("tp", t, cores, k) for k in range(1, cores)]
    def up_block(group, shard, sg):
        row = pl.multiple_of((group * shards + shard) * own_rows, own_rows)
        return su.at[pl.ds(row, own_rows), pl.ds(pl.multiple_of(sg * segment, segment), segment)]

    def up_group(group, sg):
        row = pl.multiple_of(group * group_rows, group_rows)
        return su.at[pl.ds(row, group_rows), pl.ds(sg * segment, segment)]

    def down_block(group, core):
        row = pl.multiple_of(group * segment, segment)
        return sd.at[pl.ds(row, segment), pl.ds(pl.multiple_of(core * dcols, dcols), dcols)]

    def down_piece(group, core, q):
        row = pl.multiple_of(group * segment, segment)
        return sd.at[pl.ds(row, segment), pl.ds(pl.multiple_of(core * dcols + q * tile, tile), tile)]

    def owner(sg):
        return (sg * shards + f) // nseg

    sends = []

    def begin(copy):
        copy.start()
        sends.append(copy)

    def listed(j, middle_rows, end_rows):
        r, i = j // inner, lax.rem(j, inner)
        if outer == 4:
            rows_z = [jnp.where(middle, z + a * inward, z + b * inward) for a, b in zip(middle_rows, end_rows)]
        else:
            rows_z = [lax.rem(z + d, outer) for d in range(outer)]
        at = rows_z[0]
        for d in range(1, outer):
            at = jnp.where(r == d, rows_z[d], at)
        return at * inner + lax.rem(y + i, inner)

    loads = [pltpu.make_async_copy(down_in, wide_down, load.at[0]),
             pltpu.make_async_copy(gain, scale, load.at[1]),
             pltpu.make_async_copy(tokens, raw, load.at[2])]

    def load_segment(i):
        cols = pl.ds(pl.multiple_of(i * segment, segment), segment)
        return pltpu.make_async_copy(up_in.at[:, cols], wide_up.at[:, cols], load_up.at[i])

    def target(j):
        return listed(j, (2, -1, 0, 1), (3, 2, 0, 1)) if nseg == shards else lax.rem(f + j, nseg)

    def start_load(j, carry):
        load_segment(target(j)).start()
        return carry

    for k in (2, 1, 0):
        loads[k].start()
    lax.fori_loop(0, nseg, start_load, 0)

    barrier = pltpu.get_barrier_semaphore()
    for peer in peers:
        pl.semaphore_signal(barrier, inc=1, device_id=peer, device_id_type=MESH)

    loads[2].wait()

    def norm(r, carry):
        at = pl.ds(pl.multiple_of(r * STEP, STEP), STEP)
        value = raw[at, :].astype(jnp.float32)
        inverse = lax.rsqrt(jnp.mean(value * value, axis=1, keepdims=True) + 1e-06)
        tok[at, :] = (value * inverse).astype(jnp.bfloat16)
        return carry

    lax.fori_loop(0, rows // STEP, norm, 0)

    loads[0].wait()

    def round_down(r, carry):
        row = pl.multiple_of(r * STEP, STEP)
        sd[pl.ds(pl.multiple_of(g * segment + row, STEP), STEP), pl.ds(pl.multiple_of(t * dcols, dcols), dcols)] = (
            wide_down[pl.ds(row, STEP), :].astype(jnp.bfloat16))
        return carry

    lax.fori_loop(0, segment // STEP, round_down, 0)
    loads[1].wait()
    shape = (own_rows, own_rows)
    diagonal = lax.broadcasted_iota(jnp.int32, shape, 0) == lax.broadcasted_iota(jnp.int32, shape, 1)
    column = jnp.sum(jnp.where(diagonal, scale[...], 0.0), axis=1, keepdims=True)
    pl.semaphore_wait(barrier, len(peers))

    def down_copy(k, q):
        block = down_piece(g, t, q)
        return rdma(block, block, gd_send.at[k, q], gd_recv.at[k, q], to("gr", g, groups, k))

    def down_sent(q):
        for k in range(1, groups):
            begin(down_copy(k, q))

    early_cuts = max(1, cuts // 2)
    for q in range(early_cuts):
        down_sent(q)

    pieces = [(0, half), (half, heavy - half), (heavy, front - heavy)]

    def apart(distance):
        low_way, high_way = outer - distance, distance
        return jnp.where(near_low, low_way, high_way), jnp.where(near_low, high_way, low_way)

    def hop(o, way, c):
        start, count = pieces[c]
        step = -inward if way else inward
        n = lax.rem(o + step + outer, outer)
        return rdma(span(tok, o * stack + start, count), span(tok, n * stack + start, count),
                    hop_send.at[o, way, c], hop_recv.at[n, c], beside(step))

    parts = (0, 1)
    hops = []

    def move(o, way, which, when):
        for c in which:
            if c < len(pieces):
                pl.when(when)(lambda c=c: hop(o, way, c).start())
                hops.append((o, way, c, when))

    def arrive(o, which, when, way=None):
        for c in which:
            if c < len(pieces):
                start, count = pieces[c]

                @pl.when(when)
                def _(c=c, start=start, count=count):
                    block = span(tok, o * stack + start, count)
                    rdma(block, block, hop_send.at[0, 0, c], hop_recv.at[o, c], beside(0 * z + inward)).wait_recv()

                if way is not None:
                    move(o, way, (c,), when)
                if c in parts:
                    @pl.when(when)
                    def _(c=c):
                        for i in range(1, inner):
                            heavy_copy(o, i, c).start()

    def light_copy(i):
        return rdma(span(tok, heavy, light), span(tok, rows + (i - 1) * light, light),
                    light_send.at[i], light_recv.at[i], ahead(i))

    def heavy_copy(n, i, c):
        start = 0 if c == 0 else half
        count = min(half, heavy) if c == 0 else heavy - half
        src = span(tok, n * stack + start, count)
        return rdma(src, span(tok, n * stack + front + (i - 1) * heavy + start, count),
                    heavy_send.at[n, i, c], heavy_recv.at[n, i, c], ahead(i))


    def up_copy(i):
        number = t * nseg + i
        shard, sg = lax.rem(number, shards), number // shards
        step = lax.rem(shard - f + shards, shards)
        src = up.at[:, pl.ds(pl.multiple_of(i * segment, segment), segment)]
        remote = rdma(src, up_block(g, f, sg), up_send.at[i], up_recv.at[sg, step], {"fs": shard})
        return shard == f, sg, remote

    def start_up(j, carry):
        i = target(j)
        mine, sg, remote = up_copy(i)
        load_segment(i).wait()
        cols = pl.ds(pl.multiple_of(i * segment, segment), segment)
        value = (wide_up[:, cols] * column).astype(jnp.bfloat16)
        up[:, cols] = value

        @pl.when(mine)
        def _():
            row = pl.multiple_of((g * shards + f) * own_rows, own_rows)
            su[pl.ds(row, own_rows), pl.ds(pl.multiple_of(sg * segment, segment), segment)] = value

        pl.when(jnp.logical_not(mine))(remote.start)
        return carry

    zero = z * 0
    in_one, out_one = apart(1)
    first_part = inner if nseg == shards else nseg
    last_part = shards - inner if nseg == shards else nseg
    move(zero, 0, (0,), z >= 0)
    if light:
        for i in range(1, inner):
            begin(light_copy(i))
    lax.fori_loop(0, first_part, start_up, 0)
    move(zero, 0, (1,), middle)
    lax.fori_loop(first_part, last_part, start_up, 0)
    move(zero, 1, (0,), middle)
    for c in parts:
        for i in range(1, inner):
            begin(heavy_copy(0, i, c))
    for k in range(1, cores):
        block = down_block(g, t)
        begin(rdma(block, block, ou_down_send.at[k], ou_down_recv.at[k], to("tp", t, cores, k)))

    def down_rest():
        for q in range(early_cuts, cuts):
            for k in range(1, groups):
                down_copy(k, q).start()

    def forward(first, last):
        def of_segment(sg):
            def arrived(j, carry):
                shard = listed(j, (0, 2, -1, 1), (0, 1, 2, 3))
                k = lax.rem(f - shard + shards, shards)
                block = up_block(g, shard, sg)

                @pl.when(k > 0)
                def _():
                    rdma(block, block, up_send.at[0], up_recv.at[sg, k], {"fs": shard}).wait_recv()

                for d in range(1, groups):
                    rdma(block, block, gu_send.at[sg, d, k], gu_recv.at[sg, d, k],
                         to("gr", g, groups, d)).start()
                return carry

            lax.fori_loop(first, last, arrived, 0)
            if last == shards:
                whole = up_group(g, sg)
                for c in range(1, cores):
                    rdma(whole, whole, tu_send.at[sg, 0, c], tu_recv.at[sg, 0], to("tp", t, cores, c)).start()

        for sg in range(groups):
            pl.when(owner(sg) == t)(lambda sg=sg: of_segment(sg))

    forward(0, 1)
    if light:
        for i in range(1, inner):
            light_copy(i).wait_recv()
    move(zero, 0, (2,), middle)
    lax.fori_loop(last_part, nseg, start_up, 0)
    move(zero, 0, (1, 2), end)
    forward(1, inner)
    if outer == 4:
        pl.when(end)(lambda: forward(inner, shards))
        in_two, in_three = apart(2)[0], apart(3)[0]
        arrive(out_one, (0,), middle, 0)
        arrive(in_one, (0,), middle, 1)
        arrive(in_one, (0,), end)
    if outer == 4:
        pl.when(middle)(lambda: forward(inner, 3 * inner))
        pl.when(middle)(down_rest)
    else:
        forward(inner, shards)

    if outer == 4:
        order = [jnp.where(middle, a, b) for a, b in
                 ((in_one, in_two), (in_two, in_three), (out_one, in_one), (zero, zero))]
        arrive(in_one, (1,), middle, 1)
        arrive(order[0], (2,), middle, 1)
        move(zero, 1, (1,), middle)
        arrive(out_one, (1, 2), middle, 0)
        pl.when(middle)(lambda: forward(3 * inner, shards))
        arrive(in_two, (0,), middle, 1)
        arrive(in_two, (0,), end)
        pl.when(end)(down_rest)
        arrive(in_two, (1,), end)

    def down_on(q):
        for k in range(1, groups):
            source = lax.rem(g + groups - k, groups)
            block = down_piece(source, t, q)
            rdma(block, block, gd_send.at[k, q], gd_recv.at[k, q], {"gr": source}).wait_recv()
            for c in range(1, cores):
                begin(rdma(block, block, td_send.at[c, k, q], td_recv.at[c, k, q], to("tp", t, cores, c)))

    def down_here(q):
        for c in range(1, cores):
            core = lax.rem(t + cores - c, cores)
            for k in range(1, groups):
                block = down_piece(lax.rem(g + groups - k, groups), core, q)
                rdma(block, block, td_send.at[c, k, q], td_recv.at[c, k, q], {"tp": core}).wait_recv()

    for q in range(early_cuts):
        down_on(q)

    for sg in range(groups):
        def relay(sg=sg):
            for d in range(1, groups):
                source = lax.rem(g + groups - d, groups)

                def arrived(j, carry):
                    shard = listed(j, (0, 2, -1, 1), (0, 1, 2, 3))
                    k = lax.rem(f - shard + shards, shards)
                    block = up_block(source, shard, sg)
                    rdma(block, block, gu_send.at[sg, d, k], gu_recv.at[sg, d, k], {"gr": source}).wait()
                    for c in range(1, cores):
                        rdma(block, block, ou_send.at[sg, d, c, k], ou_recv.at[sg, d, k],
                             to("tp", t, cores, c)).start()
                    return carry

                lax.fori_loop(0, shards, arrived, 0)

        pl.when(owner(sg) == t)(relay)

    for c in range(1, cores):
        core = lax.rem(t + cores - c, cores)
        block = down_block(g, core)
        rdma(block, block, ou_down_send.at[c], ou_down_recv.at[c], {"tp": core}).wait_recv()
    for sg in range(groups):
        def take(sg=sg):
            whole = up_group(g, sg)
            rdma(whole, whole, tu_send.at[sg, 0, 1], tu_recv.at[sg, 0], {"tp": owner(sg)}).wait_recv()
            for d in range(1, groups):
                def taken(k, carry):
                    block = up_block(lax.rem(g + groups - d, groups), lax.rem(f + shards - k, shards), sg)
                    rdma(block, block, tu_send.at[sg, 0, 1], ou_recv.at[sg, d, k],
                         {"tp": owner(sg)}).wait_recv()
                    return carry

                lax.fori_loop(0, shards, taken, 0)

        pl.when(owner(sg) != t)(take)

    def near_copy(o, i, n):
        return rdma(span(part, o * stack + front + (i - 1) * heavy, heavy, n),
                    span(got, (o * (inner - 1) + i - 1) * heavy, heavy, n),
                    near_send.at[o, i, n], near_recv.at[o, i, n], back(i))

    def far_copy(o, n):
        right = o > z
        step = jnp.where(right, 1, -1)
        last = jnp.where(right, o == outer - 1, o == 1)
        slot = jnp.where(last, jnp.where(right, 0, outer), o + step)
        return rdma(span(part, o * stack, front, n), span(far, slot * front, front, n),
                    far_send.at[o, n], far_recv.at[slot, n], beside(step))

    def far_arrived(slot, step, n):
        block = span(far, slot * front, front, n)
        rdma(block, block, far_send.at[0, 0], far_recv.at[slot, n], beside(step)).wait_recv()

    def clear(slot):
        def zero(r, carry):
            far[pl.ds(pl.multiple_of(slot * front + r * STEP, STEP), STEP), :] = jnp.zeros((STEP, depth), jnp.bfloat16)
            return carry

        lax.fori_loop(0, front // STEP, zero, 0)

    def passes(o):
        right = o > z
        return (right & low) | (jnp.logical_not(right) & high)

    pl.when(jnp.logical_not(low))(lambda: clear(0))
    pl.when(jnp.logical_not(high))(lambda: clear(outer))

    def tile_of(s):
        return lax.rem(s, cores) * cuts + s // cores

    def hide(o):
        for i in range(1, inner):
            for c in parts:
                start = 0 if c == 0 else half
                count = min(half, heavy) if c == 0 else heavy - half
                block = span(tok, o * stack + front + (i - 1) * heavy + start, count)
                rdma(block, block, heavy_send.at[o, i, c], heavy_recv.at[o, i, c], back(i)).wait_recv()
        both = pl.ds(pl.multiple_of(o * stack, stack), stack)

        def first(n, carry):
            cols = pl.ds(pl.multiple_of(n * TILE, TILE), TILE)
            product = jnp.dot(tok[both, :], su[:, cols], preferred_element_type=jnp.float32)
            product = jnp.maximum(product, 0.0)
            hid[:, cols] = (product * product).astype(jnp.bfloat16)
            return carry

        lax.fori_loop(0, width // TILE, first, 0)

    def project(o, start, stop):
        both = pl.ds(pl.multiple_of(o * stack, stack), stack)

        def second(s, carry):
            n = tile_of(s)
            cols = pl.ds(pl.multiple_of(n * tile, tile), tile)
            product = jnp.dot(hid[...], sd[:, cols], preferred_element_type=jnp.float32)
            part[both, cols] = product.astype(jnp.bfloat16)
            for i in range(1, inner):
                near_copy(o, i, n).start()
            return carry

        lax.fori_loop(start, stop, second, 0)

    def compute(o):
        hide(o)
        project(o, 0, tiles)

    def gather(o, n):
        for i in range(1, inner):
            near_copy(o, i, n).wait()

    def cells(start, n):
        return pl.ds(pl.multiple_of(start, STEP), STEP), pl.ds(pl.multiple_of(n * tile, tile), tile)

    def value_at(o, r, n, ends, spread):
        value = part[cells(o * stack + r * STEP, n)].astype(jnp.float32)
        if spread:
            for i in range(1, inner):
                value += got[cells((o * (inner - 1) + i - 1) * heavy + r * STEP, n)].astype(jnp.float32)
        for end in ends:
            value += far[cells(end * front + r * STEP, n)].astype(jnp.float32)
        return value

    def add_tile(o, n):
        gather(o, n)

        def sums(ends):
            def chunk(spread, r, carry):
                value = value_at(o, r, n, ends, spread)
                part[cells(o * stack + r * STEP, n)] = value.astype(jnp.bfloat16)
                return carry

            lax.fori_loop(0, heavy // STEP, functools.partial(chunk, True), 0)
            if ends:
                lax.fori_loop(heavy // STEP, front // STEP, functools.partial(chunk, False), 0)

        @pl.when(passes(o))
        def _():
            far_arrived(o, jnp.where(o > z, -1, 1), n)
            sums((o,))

        pl.when(jnp.logical_not(passes(o)))(lambda: sums(()))
        far_copy(o, n).start()

    def add(first, then, start, stop):
        lag = 0 if then is None else LAG

        def tile_sums(s, carry):
            pl.when(s < stop)(lambda: add_tile(first, tile_of(s)))
            if then is not None:
                pl.when(middle & (s >= start + lag))(lambda: add_tile(then, tile_of(s - lag)))
            return carry

        lax.fori_loop(start, stop + lag, tile_sums, 0)

    def beside_sums(o, later):
        def step(s, carry):
            pl.when(s < tiles)(lambda: add_tile(o, tile_of(s)))
            pl.when(s >= BEHIND)(lambda: project(later, s - BEHIND, s - BEHIND + 1))
            return carry

        lax.fori_loop(0, tiles + BEHIND, step, 0)

    def wait_far():
        def gone(s, carry):
            far_copy(in_three, tile_of(s)).wait_send()
            return carry

        lax.fori_loop(0, tiles - 1, gone, 0)

    ready = early_cuts * cores
    if outer == 4:
        for q in range(early_cuts):
            down_here(q)
        arrive(order[0], (2,), end)
        arrive(in_two, (1,), middle, 1)
        hide(order[0])
        project(order[0], 0, ready)
        arrive(in_one, (1,), end)
        arrive(in_three, (0,), end)
        arrive(in_two, (2,), middle, 1)
        move(zero, 1, (2,), middle)
        for q in range(early_cuts, cuts):
            down_on(q)
        for q in range(early_cuts, cuts):
            down_here(q)
        project(order[0], ready, tiles)
        arrive(in_three, (1,), end)
        pl.when(end)(lambda: add(order[0], None, 0, ready))
        pl.when(end)(lambda: add(order[0], None, ready, tiles))
        arrive(in_three, (2,), end)
        compute(order[1])

        @pl.when(middle)
        def _():
            add(order[0], None, 0, tiles // 2)
            compute(order[2])
            add(order[0], None, tiles // 2, tiles)
            compute(order[3])
            add(in_two, out_one, 0, tiles)

        arrive(in_one, (2,), end)

        @pl.when(end)
        def _():
            hide(order[2])
            beside_sums(in_three, order[2])
            hide(order[3])
            wait_far()
            beside_sums(order[2], order[3])

    else:
        raise NotImplementedError("rows along z")

    def lit_copy(i, n):
        return rdma(span(part, rows + (i - 1) * light, light, n), span(lit, (i - 1) * light, light, n),
                    lit_send.at[i, n], lit_recv.at[i, n], back(i))

    def total(s, carry):
        n = tile_of(s)
        gather(0, n)
        pl.when(low)(lambda: far_arrived(0, -1, n))
        pl.when(high)(lambda: far_arrived(outer, 1, n))
        ends = (0, outer)

        def others(r, carry):
            part[cells(r * STEP, n)] = value_at(0, r, n, ends, False).astype(jnp.bfloat16)
            return carry

        def half_done(r, carry):
            rest[cells((r * STEP - heavy), n)] = value_at(0, r, n, ends, False)
            return carry

        def done(r, carry):
            served[cells(r * STEP, n)] = value_at(0, r, n, ends, True).astype(jnp.bfloat16)
            return carry

        if light:
            lax.fori_loop(rows // STEP, front // STEP, others, 0)
            for i in range(1, inner):
                lit_copy(i, n).start()
            lax.fori_loop(heavy // STEP, rows // STEP, half_done, 0)
        lax.fori_loop(0, heavy // STEP, done, 0)
        return carry

    lax.fori_loop(0, tiles, total, 0)

    if light:
        def finish(s, carry):
            n = tile_of(s)

            for i in range(1, inner):
                lit_copy(i, n).wait()

            def chunk(r, carry):
                value = rest[cells(r * STEP, n)]
                for i in range(1, inner):
                    value += lit[cells((i - 1) * light + r * STEP, n)].astype(jnp.float32)
                served[cells(heavy + r * STEP, n)] = value.astype(jnp.bfloat16)
                return carry

            lax.fori_loop(0, light // STEP, chunk, 0)
            return carry

        lax.fori_loop(0, tiles, finish, 0)

    for o, way, c, when in hops:
        pl.when(when)(lambda o=o, way=way, c=c: hop(o, way, c).wait_send())
    for n in range(1, outer):
        for c in parts:
            for i in range(1, inner):
                heavy_copy(n, i, c).wait_send()

        def gone(m, carry, n=n):
            waited = end & (n == apart(3)[0]) & (m != tile_of(tiles - 1))
            pl.when(jnp.logical_not(waited))(lambda: far_copy(n, m).wait_send())
            return carry

        lax.fori_loop(0, tiles, gone, 0)
    for copy in sends:
        copy.wait_send()
    for q in range(early_cuts, cuts):
        for k in range(1, groups):
            down_copy(k, q).wait_send()

    def end_up(j, carry):
        mine, sg, remote = up_copy(j)
        pl.when(jnp.logical_not(mine))(remote.wait_send)
        return carry

    lax.fori_loop(0, nseg, end_up, 0)
    for sg in range(groups):
        def end(sg=sg):
            whole = up_group(g, sg)
            for c in range(1, cores):
                rdma(whole, whole, tu_send.at[sg, 0, c], tu_recv.at[sg, 0],
                     to("tp", t, cores, c)).wait_send()
            for d in range(1, groups):
                def left(k, carry):
                    block = up_block(lax.rem(g + groups - d, groups), lax.rem(f + shards - k, shards), sg)
                    for c in range(1, cores):
                        rdma(block, block, ou_send.at[sg, d, c, k], ou_recv.at[sg, d, k],
                             to("tp", t, cores, c)).wait_send()
                    return carry

                lax.fori_loop(0, shards, left, 0)

        pl.when(owner(sg) == t)(end)


def body(tokens, norm_gain, up_weight, down_weight):
    groups, shards, cores = (lax.axis_size(a) for a in ("gr", "fs", "tp"))
    segment = down_weight.shape[0]
    rows, depth = tokens.shape
    inner = inner_size(shards)
    outer = shards // inner
    heavy = heavy_rows(rows, inner)
    light = rows - heavy
    front = rows + (inner - 1) * light
    own_rows, columns = up_weight.shape
    nseg = columns // segment
    width = groups * segment
    dcols = down_weight.shape[1]
    tile = min(TILE, dcols)
    tiles = depth // tile
    cuts = dcols // tile
    bf = jnp.bfloat16
    dma = pltpu.SemaphoreType.DMA
    vmem = pl.BlockSpec(memory_space=pltpu.VMEM)
    served, su, sd = pl.pallas_call(
        functools.partial(kernel, (groups, shards, cores)),
        out_shape=(
            jax.ShapeDtypeStruct((rows, depth), bf),
            jax.ShapeDtypeStruct((depth, width), bf),
            jax.ShapeDtypeStruct((width, depth), bf),
        ),
        in_specs=[pl.BlockSpec(memory_space=pltpu.HBM)] * 4,
        out_specs=(vmem, vmem, vmem),
        scratch_shapes=[
            pltpu.VMEM((shards * rows, depth), bf),
            pltpu.VMEM((inner * rows, width), bf),
            pltpu.VMEM((shards * rows, depth), bf),
            pltpu.VMEM((max(outer * (inner - 1) * heavy, STEP), depth), bf),
            pltpu.VMEM(((outer + 1) * front, depth), bf),
            pltpu.VMEM((max((inner - 1) * light, STEP), depth), bf),
            pltpu.VMEM((max(light, STEP), depth), jnp.float32),
            pltpu.VMEM((rows, depth), bf),
            pltpu.VMEM((1, own_rows), jnp.float32),
            pltpu.VMEM((own_rows, columns), jnp.float32),
            pltpu.VMEM((segment, dcols), jnp.float32),
            pltpu.VMEM((own_rows, columns), bf),
            dma((nseg,)), dma((groups, shards)),
            dma((groups, groups, shards)), dma((groups, groups, shards)),
            dma((groups, groups, cores)), dma((groups, groups)),
            dma((groups, cuts)), dma((groups, cuts)),
            dma((cores, groups, cuts)), dma((cores, groups, cuts)),
            dma((outer, 2, 3)), dma((outer, 3)),
            dma((inner,)), dma((inner,)),
            dma((outer, inner, 2)), dma((outer, inner, 2)),
            dma((outer, inner, tiles)), dma((outer, inner, tiles)),
            dma((outer, tiles)), dma((outer + 1, tiles)),
            dma((inner, tiles)), dma((inner, tiles)),
            dma((groups, groups, cores, shards)), dma((groups, groups, shards)),
            dma((3,)), dma((nseg,)), dma((cores,)), dma((cores,)),
        ],
        compiler_params=pltpu.CompilerParams(
            collective_id=0, has_side_effects=True, vmem_limit_bytes=40 * 1024 * 1024
        ),
        name="serve",
    )(*(pltpu.with_memory_space_constraint(a, pltpu.HBM) for a in (tokens, norm_gain[None, :], up_weight, down_weight)))
    results = (served, su, sd)
    return pl.pallas_call(
        put_out,
        out_shape=tuple(jax.ShapeDtypeStruct(a.shape, a.dtype) for a in results),
        in_specs=[vmem] * 3,
        out_specs=(pl.BlockSpec(memory_space=pltpu.HBM),) * 3,
        scratch_shapes=[dma((3 * CUTS,))],
        compiler_params=pltpu.CompilerParams(vmem_limit_bytes=1 * 1024 * 1024),
        name="put_out",
    )(*results)


def put_out(*refs):
    arrays, sem = refs[:-1], refs[-1]
    half = len(arrays) // 2
    copies = []
    for src, dst in zip(arrays[:half], arrays[half:]):
        count = src.shape[0] // CUTS
        for c in range(CUTS):
            at = pl.ds(c * count, count)
            copies.append(pltpu.make_async_copy(src.at[at], dst.at[at], sem.at[len(copies)]))
    for copy in copies:
        copy.start()
    for copy in copies:
        copy.wait()


def solution(mesh):
    return jax.shard_map(
        body,
        mesh=mesh,
        in_specs=(
            P(("gr", "fs", "tp"), None),
            P(("gr", "fs")),
            P(("gr", "fs"), "tp"),
            P(("gr", "fs"), "tp"),
        ),
        out_specs=(P(("gr", "fs", "tp"), None), P(None, "fs"), P("fs", None)),
        check_vma=False,
    )
```

```python
import functools

import jax
import jax.numpy as jnp
from jax import lax
from jax.experimental import pallas as pl
from jax.experimental.pallas import tpu as pltpu
from jax.sharding import PartitionSpec as P

MESH = pl.DeviceIdType.MESH
TILE = 512
STEP = 16
LAG = 1
BEHIND = 2
HEAVY = 6
CUTS = 2


def inner_size(shards):
    return max(d for d in range(1, shards + 1) if shards % d == 0 and d * d <= shards)


def heavy_rows(rows, inner):
    return rows * HEAVY // 8 // STEP * STEP


def kernel(sizes, tokens, gain, up_in, down_in, served, su, sd, tok, hid, part, got, far, lit, rest,
           raw, scale, wide_up, wide_down, up, *sems):
    groups, shards, cores = sizes
    inner = inner_size(shards)
    outer = shards // inner
    (up_send, up_recv, gu_send, gu_recv, tu_send, tu_recv, gd_send, gd_recv,
     td_send, td_recv, hop_send, hop_recv, light_send, light_recv, heavy_send, heavy_recv,
     near_send, near_recv, far_send, far_recv, lit_send, lit_recv, ou_send, ou_recv, load, load_up, ou_down_send, ou_down_recv) = sems
    g, f, t = lax.axis_index("gr"), lax.axis_index("fs"), lax.axis_index("tp")
    z, y = f // inner, lax.rem(f, inner)
    rows, depth = raw.shape
    own_rows = up.shape[0]
    segment, dcols = wide_down.shape
    nseg = up.shape[1] // segment
    group_rows = shards * own_rows
    width = su.shape[1]
    heavy = heavy_rows(rows, inner)
    light = rows - heavy
    front = rows + (inner - 1) * light
    stack = inner * rows
    half = rows // 2
    tile = min(TILE, dcols)
    tiles = depth // tile
    cuts = dcols // tile
    low, high = z > 0, z < outer - 1
    middle, end = low & high, jnp.logical_not(low & high)
    near_low = 2 * z < outer - 1
    inward = jnp.where(near_low, 1, -1)

    def to(axis, me, size, step):
        return {axis: lax.rem(me + step, size)}

    def rdma(src, dst, send, recv, device):
        return pltpu.make_async_remote_copy(
            src_ref=src, dst_ref=dst, send_sem=send, recv_sem=recv,
            device_id=device, device_id_type=MESH,
        )

    def back(i):
        return {"fs": z * inner + lax.rem(y + inner - i, inner)}

    def ahead(i):
        return {"fs": z * inner + lax.rem(y + i, inner)}

    def beside(step):
        return {"fs": (z + step) * inner + y}

    def span(ref, start, count, n=None):
        at = pl.ds(start if isinstance(start, int) else pl.multiple_of(start, STEP), count)
        if n is None:
            return ref.at[at]
        return ref.at[at, pl.ds(n * tile if isinstance(n, int) else pl.multiple_of(n * tile, tile), tile)]

    peers = [to("fs", f, shards, k) for k in range(1, shards)]
    peers += [to("gr", g, groups, k) for k in range(1, groups)]
    peers += [to("tp", t, cores, k) for k in range(1, cores)]
    def up_block(group, shard, sg):
        row = pl.multiple_of((group * shards + shard) * own_rows, own_rows)
        return su.at[pl.ds(row, own_rows), pl.ds(pl.multiple_of(sg * segment, segment), segment)]

    def up_group(group, sg):
        row = pl.multiple_of(group * group_rows, group_rows)
        return su.at[pl.ds(row, group_rows), pl.ds(sg * segment, segment)]

    def down_block(group, core):
        row = pl.multiple_of(group * segment, segment)
        return sd.at[pl.ds(row, segment), pl.ds(pl.multiple_of(core * dcols, dcols), dcols)]

    def down_piece(group, core, q):
        row = pl.multiple_of(group * segment, segment)
        return sd.at[pl.ds(row, segment), pl.ds(pl.multiple_of(core * dcols + q * tile, tile), tile)]

    def owner(sg):
        return (sg * shards + f) // nseg

    sends = []

    def begin(copy):
        copy.start()
        sends.append(copy)

    def listed(j, middle_rows, end_rows):
        r, i = j // inner, lax.rem(j, inner)
        if outer == 4:
            rows_z = [jnp.where(middle, z + a * inward, z + b * inward) for a, b in zip(middle_rows, end_rows)]
        else:
            rows_z = [lax.rem(z + d, outer) for d in range(outer)]
        at = rows_z[0]
        for d in range(1, outer):
            at = jnp.where(r == d, rows_z[d], at)
        return at * inner + lax.rem(y + i, inner)

    loads = [pltpu.make_async_copy(down_in, wide_down, load.at[0]),
             pltpu.make_async_copy(gain, scale, load.at[1]),
             pltpu.make_async_copy(tokens, raw, load.at[2])]

    def load_segment(i):
        cols = pl.ds(pl.multiple_of(i * segment, segment), segment)
        return pltpu.make_async_copy(up_in.at[:, cols], wide_up.at[:, cols], load_up.at[i])

    def target(j):
        return listed(j, (2, -1, 0, 1), (3, 2, 0, 1)) if nseg == shards else lax.rem(f + j, nseg)

    def start_load(j, carry):
        load_segment(target(j)).start()
        return carry

    for k in (2, 1, 0):
        loads[k].start()
    lax.fori_loop(0, nseg, start_load, 0)

    barrier = pltpu.get_barrier_semaphore()
    for peer in peers:
        pl.semaphore_signal(barrier, inc=1, device_id=peer, device_id_type=MESH)

    loads[2].wait()

    def norm(r, carry):
        at = pl.ds(pl.multiple_of(r * STEP, STEP), STEP)
        value = raw[at, :].astype(jnp.float32)
        inverse = lax.rsqrt(jnp.mean(value * value, axis=1, keepdims=True) + 1e-06)
        tok[at, :] = (value * inverse).astype(jnp.bfloat16)
        return carry

    lax.fori_loop(0, rows // STEP, norm, 0)

    loads[0].wait()

    def round_down(r, carry):
        row = pl.multiple_of(r * STEP, STEP)
        sd[pl.ds(pl.multiple_of(g * segment + row, STEP), STEP), pl.ds(pl.multiple_of(t * dcols, dcols), dcols)] = (
            wide_down[pl.ds(row, STEP), :].astype(jnp.bfloat16))
        return carry

    lax.fori_loop(0, segment // STEP, round_down, 0)
    loads[1].wait()
    shape = (own_rows, own_rows)
    diagonal = lax.broadcasted_iota(jnp.int32, shape, 0) == lax.broadcasted_iota(jnp.int32, shape, 1)
    column = jnp.sum(jnp.where(diagonal, scale[...], 0.0), axis=1, keepdims=True)
    pl.semaphore_wait(barrier, len(peers))

    def down_copy(k, q):
        block = down_piece(g, t, q)
        return rdma(block, block, gd_send.at[k, q], gd_recv.at[k, q], to("gr", g, groups, k))

    def down_sent(q):
        for k in range(1, groups):
            begin(down_copy(k, q))

    early_cuts = max(1, cuts // 2)
    for q in range(early_cuts):
        down_sent(q)

    pieces = [(0, half), (half, heavy - half), (heavy, front - heavy)]

    def apart(distance):
        low_way, high_way = outer - distance, distance
        return jnp.where(near_low, low_way, high_way), jnp.where(near_low, high_way, low_way)

    def hop(o, way, c):
        start, count = pieces[c]
        step = -inward if way else inward
        n = lax.rem(o + step + outer, outer)
        return rdma(span(tok, o * stack + start, count), span(tok, n * stack + start, count),
                    hop_send.at[o, way, c], hop_recv.at[n, c], beside(step))

    parts = (0, 1)
    hops = []

    def move(o, way, which, when):
        for c in which:
            if c < len(pieces):
                pl.when(when)(lambda c=c: hop(o, way, c).start())
                hops.append((o, way, c, when))

    def arrive(o, which, when, way=None):
        for c in which:
            if c < len(pieces):
                start, count = pieces[c]

                @pl.when(when)
                def _(c=c, start=start, count=count):
                    block = span(tok, o * stack + start, count)
                    rdma(block, block, hop_send.at[0, 0, c], hop_recv.at[o, c], beside(0 * z + inward)).wait_recv()

                if way is not None:
                    move(o, way, (c,), when)
                if c in parts:
                    @pl.when(when)
                    def _(c=c):
                        for i in range(1, inner):
                            heavy_copy(o, i, c).start()

    def light_copy(i):
        return rdma(span(tok, heavy, light), span(tok, rows + (i - 1) * light, light),
                    light_send.at[i], light_recv.at[i], ahead(i))

    def heavy_copy(n, i, c):
        start = 0 if c == 0 else half
        count = min(half, heavy) if c == 0 else heavy - half
        src = span(tok, n * stack + start, count)
        return rdma(src, span(tok, n * stack + front + (i - 1) * heavy + start, count),
                    heavy_send.at[n, i, c], heavy_recv.at[n, i, c], ahead(i))


    def up_copy(i):
        number = t * nseg + i
        shard, sg = lax.rem(number, shards), number // shards
        step = lax.rem(shard - f + shards, shards)
        src = up.at[:, pl.ds(pl.multiple_of(i * segment, segment), segment)]
        remote = rdma(src, up_block(g, f, sg), up_send.at[i], up_recv.at[sg, step], {"fs": shard})
        return shard == f, sg, remote

    def start_up(j, carry):
        i = target(j)
        mine, sg, remote = up_copy(i)
        load_segment(i).wait()
        cols = pl.ds(pl.multiple_of(i * segment, segment), segment)
        value = (wide_up[:, cols] * column).astype(jnp.bfloat16)
        up[:, cols] = value

        @pl.when(mine)
        def _():
            row = pl.multiple_of((g * shards + f) * own_rows, own_rows)
            su[pl.ds(row, own_rows), pl.ds(pl.multiple_of(sg * segment, segment), segment)] = value

        pl.when(jnp.logical_not(mine))(remote.start)
        return carry

    zero = z * 0
    in_one, out_one = apart(1)
    first_part = inner if nseg == shards else nseg
    last_part = shards - inner if nseg == shards else nseg
    move(zero, 0, (0,), z >= 0)
    if light:
        for i in range(1, inner):
            begin(light_copy(i))
    lax.fori_loop(0, first_part, start_up, 0)
    move(zero, 0, (1,), middle)
    lax.fori_loop(first_part, last_part, start_up, 0)
    move(zero, 1, (0,), middle)
    for c in parts:
        for i in range(1, inner):
            begin(heavy_copy(0, i, c))
    for k in range(1, cores):
        block = down_block(g, t)
        begin(rdma(block, block, ou_down_send.at[k], ou_down_recv.at[k], to("tp", t, cores, k)))

    def down_rest():
        for q in range(early_cuts, cuts):
            for k in range(1, groups):
                down_copy(k, q).start()

    def forward(first, last):
        def of_segment(sg):
            def arrived(j, carry):
                shard = listed(j, (0, 2, -1, 1), (0, 1, 2, 3))
                k = lax.rem(f - shard + shards, shards)
                block = up_block(g, shard, sg)

                @pl.when(k > 0)
                def _():
                    rdma(block, block, up_send.at[0], up_recv.at[sg, k], {"fs": shard}).wait_recv()

                for d in range(1, groups):
                    rdma(block, block, gu_send.at[sg, d, k], gu_recv.at[sg, d, k],
                         to("gr", g, groups, d)).start()
                return carry

            lax.fori_loop(first, last, arrived, 0)
            if last == shards:
                whole = up_group(g, sg)
                for c in range(1, cores):
                    rdma(whole, whole, tu_send.at[sg, 0, c], tu_recv.at[sg, 0], to("tp", t, cores, c)).start()

        for sg in range(groups):
            pl.when(owner(sg) == t)(lambda sg=sg: of_segment(sg))

    forward(0, 1)
    if light:
        for i in range(1, inner):
            light_copy(i).wait_recv()
    move(zero, 0, (2,), middle)
    lax.fori_loop(last_part, nseg, start_up, 0)
    move(zero, 0, (1, 2), end)
    forward(1, inner)
    if outer == 4:
        pl.when(end)(lambda: forward(inner, shards))
        in_two, in_three = apart(2)[0], apart(3)[0]
        arrive(out_one, (0,), middle, 0)
        arrive(in_one, (0,), middle, 1)
        arrive(in_one, (0,), end)
    if outer == 4:
        pl.when(middle)(lambda: forward(inner, 3 * inner))
        pl.when(middle)(down_rest)
    else:
        forward(inner, shards)

    if outer == 4:
        order = [jnp.where(middle, a, b) for a, b in
                 ((in_one, in_two), (in_two, in_three), (out_one, in_one), (zero, zero))]
        arrive(in_one, (1,), middle, 1)
        arrive(order[0], (2,), middle, 1)
        move(zero, 1, (1,), middle)
        arrive(out_one, (1, 2), middle, 0)
        pl.when(middle)(lambda: forward(3 * inner, shards))
        arrive(in_two, (0,), middle, 1)
        arrive(in_two, (0,), end)
        pl.when(end)(down_rest)
        arrive(in_two, (1,), end)

    def down_on(q):
        for k in range(1, groups):
            source = lax.rem(g + groups - k, groups)
            block = down_piece(source, t, q)
            rdma(block, block, gd_send.at[k, q], gd_recv.at[k, q], {"gr": source}).wait_recv()
            for c in range(1, cores):
                begin(rdma(block, block, td_send.at[c, k, q], td_recv.at[c, k, q], to("tp", t, cores, c)))

    def down_here(q):
        for c in range(1, cores):
            core = lax.rem(t + cores - c, cores)
            for k in range(1, groups):
                block = down_piece(lax.rem(g + groups - k, groups), core, q)
                rdma(block, block, td_send.at[c, k, q], td_recv.at[c, k, q], {"tp": core}).wait_recv()

    for q in range(early_cuts):
        down_on(q)

    for sg in range(groups):
        def relay(sg=sg):
            for d in range(1, groups):
                source = lax.rem(g + groups - d, groups)

                def arrived(j, carry):
                    shard = listed(j, (0, 2, -1, 1), (0, 1, 2, 3))
                    k = lax.rem(f - shard + shards, shards)
                    block = up_block(source, shard, sg)
                    rdma(block, block, gu_send.at[sg, d, k], gu_recv.at[sg, d, k], {"gr": source}).wait()
                    for c in range(1, cores):
                        rdma(block, block, ou_send.at[sg, d, c, k], ou_recv.at[sg, d, k],
                             to("tp", t, cores, c)).start()
                    return carry

                lax.fori_loop(0, shards, arrived, 0)

        pl.when(owner(sg) == t)(relay)

    for c in range(1, cores):
        core = lax.rem(t + cores - c, cores)
        block = down_block(g, core)
        rdma(block, block, ou_down_send.at[c], ou_down_recv.at[c], {"tp": core}).wait_recv()
    for sg in range(groups):
        def take(sg=sg):
            whole = up_group(g, sg)
            rdma(whole, whole, tu_send.at[sg, 0, 1], tu_recv.at[sg, 0], {"tp": owner(sg)}).wait_recv()
            for d in range(1, groups):
                def taken(k, carry):
                    block = up_block(lax.rem(g + groups - d, groups), lax.rem(f + shards - k, shards), sg)
                    rdma(block, block, tu_send.at[sg, 0, 1], ou_recv.at[sg, d, k],
                         {"tp": owner(sg)}).wait_recv()
                    return carry

                lax.fori_loop(0, shards, taken, 0)

        pl.when(owner(sg) != t)(take)

    def near_copy(o, i, n):
        return rdma(span(part, o * stack + front + (i - 1) * heavy, heavy, n),
                    span(got, (o * (inner - 1) + i - 1) * heavy, heavy, n),
                    near_send.at[o, i, n], near_recv.at[o, i, n], back(i))

    def far_copy(o, n):
        right = o > z
        step = jnp.where(right, 1, -1)
        last = jnp.where(right, o == outer - 1, o == 1)
        slot = jnp.where(last, jnp.where(right, 0, outer), o + step)
        return rdma(span(part, o * stack, front, n), span(far, slot * front, front, n),
                    far_send.at[o, n], far_recv.at[slot, n], beside(step))

    def far_arrived(slot, step, n):
        block = span(far, slot * front, front, n)
        rdma(block, block, far_send.at[0, 0], far_recv.at[slot, n], beside(step)).wait_recv()

    def clear(slot):
        def zero(r, carry):
            far[pl.ds(pl.multiple_of(slot * front + r * STEP, STEP), STEP), :] = jnp.zeros((STEP, depth), jnp.bfloat16)
            return carry

        lax.fori_loop(0, front // STEP, zero, 0)

    def passes(o):
        right = o > z
        return (right & low) | (jnp.logical_not(right) & high)

    pl.when(jnp.logical_not(low))(lambda: clear(0))
    pl.when(jnp.logical_not(high))(lambda: clear(outer))

    def tile_of(s):
        return lax.rem(s, cores) * cuts + s // cores

    def hide(o):
        for i in range(1, inner):
            for c in parts:
                start = 0 if c == 0 else half
                count = min(half, heavy) if c == 0 else heavy - half
                block = span(tok, o * stack + front + (i - 1) * heavy + start, count)
                rdma(block, block, heavy_send.at[o, i, c], heavy_recv.at[o, i, c], back(i)).wait_recv()
        both = pl.ds(pl.multiple_of(o * stack, stack), stack)

        def first(n, carry):
            cols = pl.ds(pl.multiple_of(n * TILE, TILE), TILE)
            product = jnp.dot(tok[both, :], su[:, cols], preferred_element_type=jnp.float32)
            product = jnp.maximum(product, 0.0)
            hid[:, cols] = (product * product).astype(jnp.bfloat16)
            return carry

        lax.fori_loop(0, width // TILE, first, 0)

    def project(o, start, stop):
        both = pl.ds(pl.multiple_of(o * stack, stack), stack)

        def second(s, carry):
            n = tile_of(s)
            cols = pl.ds(pl.multiple_of(n * tile, tile), tile)
            product = jnp.dot(hid[...], sd[:, cols], preferred_element_type=jnp.float32)
            part[both, cols] = product.astype(jnp.bfloat16)
            for i in range(1, inner):
                near_copy(o, i, n).start()
            return carry

        lax.fori_loop(start, stop, second, 0)

    def compute(o):
        hide(o)
        project(o, 0, tiles)

    def gather(o, n):
        for i in range(1, inner):
            near_copy(o, i, n).wait()

    def cells(start, n):
        return pl.ds(pl.multiple_of(start, STEP), STEP), pl.ds(pl.multiple_of(n * tile, tile), tile)

    def value_at(o, r, n, ends, spread):
        value = part[cells(o * stack + r * STEP, n)].astype(jnp.float32)
        if spread:
            for i in range(1, inner):
                value += got[cells((o * (inner - 1) + i - 1) * heavy + r * STEP, n)].astype(jnp.float32)
        for end in ends:
            value += far[cells(end * front + r * STEP, n)].astype(jnp.float32)
        return value

    def add_tile(o, n):
        gather(o, n)

        def sums(ends):
            def chunk(spread, r, carry):
                value = value_at(o, r, n, ends, spread)
                part[cells(o * stack + r * STEP, n)] = value.astype(jnp.bfloat16)
                return carry

            lax.fori_loop(0, heavy // STEP, functools.partial(chunk, True), 0)
            if ends:
                lax.fori_loop(heavy // STEP, front // STEP, functools.partial(chunk, False), 0)

        @pl.when(passes(o))
        def _():
            far_arrived(o, jnp.where(o > z, -1, 1), n)
            sums((o,))

        pl.when(jnp.logical_not(passes(o)))(lambda: sums(()))
        far_copy(o, n).start()

    def add(first, then, start, stop):
        lag = 0 if then is None else LAG

        def tile_sums(s, carry):
            pl.when(s < stop)(lambda: add_tile(first, tile_of(s)))
            if then is not None:
                pl.when(middle & (s >= start + lag))(lambda: add_tile(then, tile_of(s - lag)))
            return carry

        lax.fori_loop(start, stop + lag, tile_sums, 0)

    def beside_sums(o, later):
        def step(s, carry):
            pl.when(s < tiles)(lambda: add_tile(o, tile_of(s)))
            pl.when(s >= BEHIND)(lambda: project(later, s - BEHIND, s - BEHIND + 1))
            return carry

        lax.fori_loop(0, tiles + BEHIND, step, 0)

    def wait_far():
        def gone(s, carry):
            far_copy(in_three, tile_of(s)).wait_send()
            return carry

        lax.fori_loop(0, tiles - 1, gone, 0)

    ready = early_cuts * cores
    if outer == 4:
        for q in range(early_cuts):
            down_here(q)
        arrive(order[0], (2,), end)
        arrive(in_two, (1,), middle, 1)
        hide(order[0])
        project(order[0], 0, ready)
        arrive(in_one, (1,), end)
        pl.when(end)(lambda: add(order[0], None, 0, ready))
        arrive(in_three, (0,), end)
        arrive(in_two, (2,), middle, 1)
        move(zero, 1, (2,), middle)
        for q in range(early_cuts, cuts):
            down_on(q)
        for q in range(early_cuts, cuts):
            down_here(q)
        project(order[0], ready, tiles)
        arrive(in_three, (1,), end)
        pl.when(end)(lambda: add(order[0], None, ready, tiles))
        arrive(in_three, (2,), end)
        compute(order[1])

        @pl.when(middle)
        def _():
            add(order[0], None, 0, tiles // 2)
            compute(order[2])
            add(order[0], None, tiles // 2, tiles)
            compute(order[3])
            add(in_two, out_one, 0, tiles)

        arrive(in_one, (2,), end)

        @pl.when(end)
        def _():
            hide(order[2])
            beside_sums(in_three, order[2])
            hide(order[3])
            wait_far()
            beside_sums(order[2], order[3])

    else:
        raise NotImplementedError("rows along z")

    def lit_copy(i, n):
        return rdma(span(part, rows + (i - 1) * light, light, n), span(lit, (i - 1) * light, light, n),
                    lit_send.at[i, n], lit_recv.at[i, n], back(i))

    def total(s, carry):
        n = tile_of(s)
        gather(0, n)
        pl.when(low)(lambda: far_arrived(0, -1, n))
        pl.when(high)(lambda: far_arrived(outer, 1, n))
        ends = (0, outer)

        def others(r, carry):
            part[cells(r * STEP, n)] = value_at(0, r, n, ends, False).astype(jnp.bfloat16)
            return carry

        def half_done(r, carry):
            rest[cells((r * STEP - heavy), n)] = value_at(0, r, n, ends, False)
            return carry

        def done(r, carry):
            served[cells(r * STEP, n)] = value_at(0, r, n, ends, True).astype(jnp.bfloat16)
            return carry

        if light:
            lax.fori_loop(rows // STEP, front // STEP, others, 0)
            for i in range(1, inner):
                lit_copy(i, n).start()
            lax.fori_loop(heavy // STEP, rows // STEP, half_done, 0)
        lax.fori_loop(0, heavy // STEP, done, 0)
        return carry

    lax.fori_loop(0, tiles, total, 0)

    if light:
        def finish(s, carry):
            n = tile_of(s)

            for i in range(1, inner):
                lit_copy(i, n).wait()

            def chunk(r, carry):
                value = rest[cells(r * STEP, n)]
                for i in range(1, inner):
                    value += lit[cells((i - 1) * light + r * STEP, n)].astype(jnp.float32)
                served[cells(heavy + r * STEP, n)] = value.astype(jnp.bfloat16)
                return carry

            lax.fori_loop(0, light // STEP, chunk, 0)
            return carry

        lax.fori_loop(0, tiles, finish, 0)

    for o, way, c, when in hops:
        pl.when(when)(lambda o=o, way=way, c=c: hop(o, way, c).wait_send())
    for n in range(1, outer):
        for c in parts:
            for i in range(1, inner):
                heavy_copy(n, i, c).wait_send()

        def gone(m, carry, n=n):
            waited = end & (n == apart(3)[0]) & (m != tile_of(tiles - 1))
            pl.when(jnp.logical_not(waited))(lambda: far_copy(n, m).wait_send())
            return carry

        lax.fori_loop(0, tiles, gone, 0)
    for copy in sends:
        copy.wait_send()
    for q in range(early_cuts, cuts):
        for k in range(1, groups):
            down_copy(k, q).wait_send()

    def end_up(j, carry):
        mine, sg, remote = up_copy(j)
        pl.when(jnp.logical_not(mine))(remote.wait_send)
        return carry

    lax.fori_loop(0, nseg, end_up, 0)
    for sg in range(groups):
        def end(sg=sg):
            whole = up_group(g, sg)
            for c in range(1, cores):
                rdma(whole, whole, tu_send.at[sg, 0, c], tu_recv.at[sg, 0],
                     to("tp", t, cores, c)).wait_send()
            for d in range(1, groups):
                def left(k, carry):
                    block = up_block(lax.rem(g + groups - d, groups), lax.rem(f + shards - k, shards), sg)
                    for c in range(1, cores):
                        rdma(block, block, ou_send.at[sg, d, c, k], ou_recv.at[sg, d, k],
                             to("tp", t, cores, c)).wait_send()
                    return carry

                lax.fori_loop(0, shards, left, 0)

        pl.when(owner(sg) == t)(end)


def body(tokens, norm_gain, up_weight, down_weight):
    groups, shards, cores = (lax.axis_size(a) for a in ("gr", "fs", "tp"))
    segment = down_weight.shape[0]
    rows, depth = tokens.shape
    inner = inner_size(shards)
    outer = shards // inner
    heavy = heavy_rows(rows, inner)
    light = rows - heavy
    front = rows + (inner - 1) * light
    own_rows, columns = up_weight.shape
    nseg = columns // segment
    width = groups * segment
    dcols = down_weight.shape[1]
    tile = min(TILE, dcols)
    tiles = depth // tile
    cuts = dcols // tile
    bf = jnp.bfloat16
    dma = pltpu.SemaphoreType.DMA
    vmem = pl.BlockSpec(memory_space=pltpu.VMEM)
    served, su, sd = pl.pallas_call(
        functools.partial(kernel, (groups, shards, cores)),
        out_shape=(
            jax.ShapeDtypeStruct((rows, depth), bf),
            jax.ShapeDtypeStruct((depth, width), bf),
            jax.ShapeDtypeStruct((width, depth), bf),
        ),
        in_specs=[pl.BlockSpec(memory_space=pltpu.HBM)] * 4,
        out_specs=(vmem, vmem, vmem),
        scratch_shapes=[
            pltpu.VMEM((shards * rows, depth), bf),
            pltpu.VMEM((inner * rows, width), bf),
            pltpu.VMEM((shards * rows, depth), bf),
            pltpu.VMEM((max(outer * (inner - 1) * heavy, STEP), depth), bf),
            pltpu.VMEM(((outer + 1) * front, depth), bf),
            pltpu.VMEM((max((inner - 1) * light, STEP), depth), bf),
            pltpu.VMEM((max(light, STEP), depth), jnp.float32),
            pltpu.VMEM((rows, depth), bf),
            pltpu.VMEM((1, own_rows), jnp.float32),
            pltpu.VMEM((own_rows, columns), jnp.float32),
            pltpu.VMEM((segment, dcols), jnp.float32),
            pltpu.VMEM((own_rows, columns), bf),
            dma((nseg,)), dma((groups, shards)),
            dma((groups, groups, shards)), dma((groups, groups, shards)),
            dma((groups, groups, cores)), dma((groups, groups)),
            dma((groups, cuts)), dma((groups, cuts)),
            dma((cores, groups, cuts)), dma((cores, groups, cuts)),
            dma((outer, 2, 3)), dma((outer, 3)),
            dma((inner,)), dma((inner,)),
            dma((outer, inner, 2)), dma((outer, inner, 2)),
            dma((outer, inner, tiles)), dma((outer, inner, tiles)),
            dma((outer, tiles)), dma((outer + 1, tiles)),
            dma((inner, tiles)), dma((inner, tiles)),
            dma((groups, groups, cores, shards)), dma((groups, groups, shards)),
            dma((3,)), dma((nseg,)), dma((cores,)), dma((cores,)),
        ],
        compiler_params=pltpu.CompilerParams(
            collective_id=0, has_side_effects=True, vmem_limit_bytes=40 * 1024 * 1024
        ),
        name="serve",
    )(*(pltpu.with_memory_space_constraint(a, pltpu.HBM) for a in (tokens, norm_gain[None, :], up_weight, down_weight)))
    results = (served, su, sd)
    return pl.pallas_call(
        put_out,
        out_shape=tuple(jax.ShapeDtypeStruct(a.shape, a.dtype) for a in results),
        in_specs=[vmem] * 3,
        out_specs=(pl.BlockSpec(memory_space=pltpu.HBM),) * 3,
        scratch_shapes=[dma((3 * CUTS,))],
        compiler_params=pltpu.CompilerParams(vmem_limit_bytes=1 * 1024 * 1024),
        name="put_out",
    )(*results)


def put_out(*refs):
    arrays, sem = refs[:-1], refs[-1]
    half = len(arrays) // 2
    copies = []
    for src, dst in zip(arrays[:half], arrays[half:]):
        count = src.shape[0] // CUTS
        for c in range(CUTS):
            at = pl.ds(c * count, count)
            copies.append(pltpu.make_async_copy(src.at[at], dst.at[at], sem.at[len(copies)]))
    for copy in copies:
        copy.start()
    for copy in copies:
        copy.wait()


def solution(mesh):
    return jax.shard_map(
        body,
        mesh=mesh,
        in_specs=(
            P(("gr", "fs", "tp"), None),
            P(("gr", "fs")),
            P(("gr", "fs"), "tp"),
            P(("gr", "fs"), "tp"),
        ),
        out_specs=(P(("gr", "fs", "tp"), None), P(None, "fs"), P("fs", None)),
        check_vma=False,
    )
```
